512 devices in a mesh: grp: 2 (over y), sp: 16 (over z), tp: 16 (over x, core).
Axes of the slice: x: 8, y: 2, z: 16, core: 2. Of those that a mesh axis runs over, the one named last changes fastest.
The devices are a block of a 8x8x16 slice.
Arguments:
- target: bfloat16 [8192, 2048], P(('grp', 'sp', 'tp')), parts along dimension 0, may hold values from -20 to 20
- source: bfloat16 [16384, 2048], P(('grp', 'sp')), parts along dimension 0, may hold values from -20 to 20
- source_gain: float32 [2048], replicated, may hold values from 0.1 to 1.9
- query_gain: float32 [2, 2048], replicated, may hold values from 0.1 to 1.9
- out_gain: float32 [2, 2048], replicated, may hold values from 0.1 to 1.9
- query_weight: bfloat16 [2, 2048, 2048], P(None, None, 'tp'), may hold values from -1 to 1
- key_weight: bfloat16 [2, 2048, 512], P(None, None, 'tp'), may hold values from -1 to 1
- value_weight: bfloat16 [2, 2048, 512], P(None, None, 'tp'), may hold values from -0.125 to 0.125
- out_weight: bfloat16 [2, 2048, 2048], P(None, 'tp'), may hold values from -0.125 to 0.125
Outputs:
- result: bfloat16 [8192, 2048], P(('grp', 'sp', 'tp')), parts along dimension 0
The draws below stay inside these ranges and needn't reach their ends.
There are 2 independent parts, one for each index of `grp`. The reference program is written for one: setup_inputs(seed, part) draws one part's arguments, and reference() takes and returns one part's arrays. A program takes and returns all parts, laid end to end along the dimension named above; an argument that names none is the same for every part. Nothing has to cross between parts.
All inputs are finite; a program needn't handle non-finite values.
Results may differ from the reference program's by a relative error of at most 0.024.
Values may be sent and summed in bfloat16 or wider, within the bound.
No kernel may reach another device: no remote copies, remote signals or barrier semaphores. Data moves between devices by JAX's collectives and lax.ppermute only.
A program may use at most 64 MiB of HBM per device.

```python
import jax
import jax.numpy as jnp
from jax import lax

D = 2048
HD = 256
QH = 8
KVH = 2
LAYERS = 2
QW = 2048
KVW = 512
SRC = 8192
TGT = 4096


def feature_rows(key, row_count):
    keys_split = jax.random.split(key, 3)
    return jax.random.truncated_normal(keys_split[2], -5.0, 5.0, (row_count, D), jnp.float32)


def drawn_weight(key, fan_rows, columns):
    return jax.random.truncated_normal(key, -5.0, 5.0, (LAYERS, fan_rows, columns), jnp.float32) * fan_rows ** (-0.5)


def draw_target(key, part):
    own_key = jax.random.fold_in(key, 101)
    return feature_rows(own_key, TGT).astype(jnp.bfloat16)


def draw_source(key, part):
    own_key = jax.random.fold_in(key, 202)
    return feature_rows(own_key, SRC).astype(jnp.bfloat16)


def draw_query_weight(key, part):
    own_key = jax.random.fold_in(key, 303)
    return drawn_weight(own_key, D, QW).astype(jnp.bfloat16)


def draw_key_weight(key, part):
    own_key = jax.random.fold_in(key, 404)
    return drawn_weight(own_key, D, KVW).astype(jnp.bfloat16)


def level_of(stream_key, extent, cuts, low, top_value):
    level, own = 1.0, jax.random.fold_in(stream_key, 6)
    for dim, shards_of in cuts:
        heights = jnp.exp(jax.random.uniform(jax.random.fold_in(own, dim), (shards_of,), jnp.float32, low / len(cuts), top_value / len(cuts)))
        level = level * jnp.repeat(heights, extent[dim] // shards_of).reshape([-1 if axis == dim else 1 for axis in range(len(extent))])
    return level


def gaussian(stream_key, shape, spread, bound, pieces=(), kind=jnp.bfloat16):
    level = level_of(stream_key, shape, pieces, -0.22, 0.18) if pieces else 1.0
    drawn = jax.random.normal(stream_key, shape, jnp.float32) * spread * level
    return jnp.minimum(jnp.maximum(drawn, -bound), bound).astype(kind)


def setup_inputs(seed: int = 0, part: int = 0) -> dict:
    arg_keys = jax.random.split(jax.random.key(seed), 10)
    own_keys = jax.random.split(jax.random.fold_in(arg_keys[9], part), 10)
    return {
        "target": draw_target(jax.random.fold_in(jax.random.fold_in(arg_keys[9], part), 71), part),
        "source": draw_source(jax.random.fold_in(jax.random.fold_in(arg_keys[9], part), 71), part),
        "source_gain": jnp.clip(1.0 + 0.18 * jax.random.normal(arg_keys[2], (D,), jnp.float32), 0.1, 1.9),
        "query_gain": jnp.clip(1.0 + 0.18 * jax.random.normal(arg_keys[3], (LAYERS, D), jnp.float32), 0.1, 1.9),
        "out_gain": jnp.clip(1.0 + 0.18 * jax.random.normal(arg_keys[4], (LAYERS, D), jnp.float32), 0.1, 1.9),
        "query_weight": draw_query_weight(jax.random.fold_in(arg_keys[9], 71), part),
        "key_weight": draw_key_weight(jax.random.fold_in(arg_keys[9], 71), part),
        "value_weight": gaussian(arg_keys[7], (LAYERS, D, KVW), D ** -0.5, 0.125, ((2, 16),)),
        "out_weight": gaussian(arg_keys[8], (LAYERS, QW, D), QW ** -0.5, 0.125, ((1, 16),)),
    }


EPSILON = 1e-06

def rms_scaled(matrix_rows, gain_row):
    values = matrix_rows.astype(jnp.float32)
    inverse = lax.rsqrt(lax.optimization_barrier(jnp.mean(values * values, axis=-1, keepdims=True)) + EPSILON)
    return values * inverse * gain_row.astype(jnp.float32)

def reference(target, source, source_gain, query_gain, out_gain, query_weight, key_weight, value_weight, out_weight):
    normed_source = rms_scaled(source, source_gain).astype(jnp.bfloat16)
    heads_per_group = QH // KVH
    score_scale = HD ** (-0.5)
    residual = target
    for layer_index in range(LAYERS):
        all_keys = jnp.dot(normed_source, key_weight[layer_index], preferred_element_type=jnp.float32).astype(jnp.bfloat16)
        all_values = jnp.dot(normed_source, value_weight[layer_index], preferred_element_type=jnp.float32).astype(jnp.bfloat16)
        normed = rms_scaled(residual, query_gain[layer_index]).astype(jnp.bfloat16)
        queries = jnp.dot(normed, query_weight[layer_index], preferred_element_type=jnp.float32).astype(jnp.bfloat16)

        def one_head(head_index):
            key_head = head_index // heads_per_group
            query_rows = lax.dynamic_slice_in_dim(queries, head_index * HD, HD, 1)
            key_rows = lax.dynamic_slice_in_dim(all_keys, key_head * HD, HD, 1)
            value_rows = lax.dynamic_slice_in_dim(all_values, key_head * HD, HD, 1)
            scores = jnp.dot(query_rows, key_rows.T, preferred_element_type=jnp.float32) * score_scale
            row_peak = lax.optimization_barrier(jnp.max(scores, axis=1, keepdims=True))
            weights = jnp.exp(scores - row_peak)
            row_total = lax.optimization_barrier(jnp.sum(weights, axis=1, keepdims=True))
            mixed_rows = jnp.dot(weights.astype(jnp.bfloat16), value_rows, preferred_element_type=jnp.float32)
            return (mixed_rows / row_total).astype(jnp.bfloat16)
        head_outputs = lax.map(one_head, jnp.arange(QH, dtype=jnp.int32))
        attended = jnp.transpose(head_outputs, (1, 0, 2)).reshape(queries.shape[0], QH * HD)
        projected = jnp.dot(attended, out_weight[layer_index], preferred_element_type=jnp.float32)
        residual = (residual.astype(jnp.float32) + rms_scaled(projected, out_gain[layer_index])).astype(jnp.bfloat16)
    return residual
```

```python
import jax
import jax.numpy as jnp
from jax import lax
from jax.experimental import pallas as pl
from jax.experimental.pallas import tpu as pltpu
from jax.sharding import Mesh
from jax.sharding import PartitionSpec as P

HD = 256
QH = 8
KVH = 2
LAYERS = 2
HERE = QH // KVH
EPSILON = 1e-06
STATS = 16

CHIPS = ("kv", "quarter")
GROUP = ("quarter", "core")
BF16 = jnp.bfloat16
F32 = jnp.float32


def dot(a, b, contract=((1,), (0,))):
    return lax.dot_general(a, b, (contract, ((), ())), preferred_element_type=F32)


def scaled(values, gain):
    inverse = lax.rsqrt(jnp.mean(values * values, axis=-1, keepdims=True) + EPSILON)
    return values * inverse * gain


def held_in_vmem(*arrays):
    return [pltpu.with_memory_space_constraint(a, pltpu.VMEM) for a in arrays]


def vmem_out(shape):
    return pltpu.VMEM(tuple(shape), BF16)


def in_vmem(count):
    return [pl.BlockSpec(memory_space=pltpu.VMEM)] * count


def source_kernel(source_ref, gain_ref, key_ref, value_ref, out_ref, weight_ref):
    width = key_ref.shape[2]

    @pl.when(pl.program_id(0) == 0)
    def _():
        for layer in range(LAYERS):
            weight_ref[:, layer * width : (layer + 1) * width] = key_ref[layer]
            weight_ref[:, (LAYERS + layer) * width : (LAYERS + layer + 1) * width] = value_ref[layer]

    normed = scaled(source_ref[...].astype(F32), gain_ref[...]).astype(BF16)
    columns = dot(normed, weight_ref[...]).T.astype(BF16)
    out_ref[...] = columns.reshape(out_ref.shape)


def source_columns(source, gain, key_weight, value_weight, quarters):
    rows, features = source.shape
    width = key_weight.shape[2]
    block = rows // quarters
    return pl.pallas_call(
        source_kernel,
        grid=(quarters,),
        in_specs=[
            pl.BlockSpec((block, features), lambda i: (i, 0)),
            pl.BlockSpec((1, features), lambda i: (0, 0)),
            pl.BlockSpec(key_weight.shape, lambda i: (0, 0, 0)),
            pl.BlockSpec(value_weight.shape, lambda i: (0, 0, 0)),
        ],
        out_specs=pl.BlockSpec((1, 2, LAYERS * width, block), lambda i: (i, 0, 0, 0)),
        out_shape=jax.ShapeDtypeStruct((quarters, 2, LAYERS * width, block), BF16),
        scratch_shapes=[pltpu.VMEM((features, 2 * LAYERS * width), BF16)],
        name="source_columns",
    )(source, gain, key_weight, value_weight)


def norm_kernel(rows_ref, gain_ref, out_ref):
    out_ref[...] = scaled(rows_ref[...].astype(F32), gain_ref[...]).astype(BF16)


def first_norm(rows, gain):
    return pl.pallas_call(
        norm_kernel,
        in_specs=in_vmem(2),
        out_specs=in_vmem(1)[0],
        out_shape=vmem_out(rows.shape),
        name="first_norm",
    )(*held_in_vmem(rows, gain))


def query_kernel(core_ref, rows_ref, mine_ref, other_ref, out_ref):
    chips, block, features = rows_ref.shape
    rows = rows_ref[...].reshape(chips * block, features)
    mine = dot(rows, mine_ref[...]).astype(BF16)
    other = dot(rows, other_ref[...]).astype(BF16)
    first = core_ref[0] == 0
    width = mine.shape[1]
    out_ref[:, :width] = jnp.where(first, mine, other)
    out_ref[:, width:] = jnp.where(first, other, mine)


def project_queries(core, rows, mine, other):
    chips, block, _ = rows.shape
    return pl.pallas_call(
        query_kernel,
        in_specs=[pl.BlockSpec(memory_space=pltpu.SMEM)] + in_vmem(3),
        out_specs=in_vmem(1)[0],
        out_shape=vmem_out((chips * block, 2 * mine.shape[1])),
        name="project_queries",
    )(core, *held_in_vmem(rows, mine, other))


def attend_kernel(core_ref, query_ref, mine_ref, other_ref, out_ref, score_ref):
    heads, rows, width = query_ref.shape
    blocks, _, block = mine_ref.shape
    queries = query_ref[...].reshape(heads * rows, width)
    scale = width ** (-0.5)

    def work(key_ref, value_ref):
        peak = None
        for b in range(0, blocks, 2):
            keys = jnp.concatenate([key_ref[b], key_ref[b + 1]], axis=1)
            scores = dot(queries, keys) * scale
            score_ref[:, b * block : (b + 2) * block] = scores
            top = jnp.max(scores, axis=1, keepdims=True)
            peak = top if peak is None else jnp.maximum(peak, top)
        total, mixed = None, None
        for b in range(0, blocks, 2):
            values = jnp.concatenate([value_ref[b], value_ref[b + 1]], axis=1)
            weights = jnp.exp(score_ref[:, b * block : (b + 2) * block] - peak)
            part = jnp.sum(weights, axis=1, keepdims=True)
            share = dot(weights.astype(BF16), values, ((1,), (1,)))
            total = part if total is None else total + part
            mixed = share if mixed is None else mixed + share
        out_ref[:, :rows, :] = (mixed / total).astype(BF16).reshape(heads, rows, width)
        level = peak + jnp.log(total)
        high = level.astype(BF16).astype(F32)
        low = level - high
        for h in range(heads):
            for part, at in ((high, 0), (low, rows)):
                column = jnp.broadcast_to(part[h * rows : (h + 1) * rows], (rows, rows))
                out_ref[h, rows:, at : at + rows] = column.T[:STATS].astype(BF16)

    @pl.when(core_ref[0] == 0)
    def _():
        work(mine_ref, other_ref)

    @pl.when(core_ref[0] != 0)
    def _():
        work(other_ref, mine_ref)


def attend(core, queries, mine, other):
    heads, rows, width = queries.shape
    blocks, _, block = mine.shape
    return pl.pallas_call(
        attend_kernel,
        in_specs=[pl.BlockSpec(memory_space=pltpu.SMEM)] + in_vmem(3),
        out_specs=in_vmem(1)[0],
        out_shape=vmem_out((heads, rows + STATS, width)),
        scratch_shapes=[pltpu.VMEM((heads * rows, blocks * block), F32)],
        name="attend",
    )(core, *held_in_vmem(queries, mine, other))


def merge_kernel(core_ref, part_ref, mine_ref, other_ref, out_ref):
    parts, extended, width = part_ref.shape
    rows = extended - STATS
    levels = []
    for s in range(parts):
        stats = part_ref[s, rows:, :].astype(F32)
        line = stats[:1, :rows] + stats[:1, rows:]
        levels.append(jnp.broadcast_to(line, (rows, rows)).T)
    peak = levels[0]
    for level in levels[1:]:
        peak = jnp.maximum(peak, level)
    shares = [jnp.exp(level - peak) for level in levels]
    total = shares[0]
    for share in shares[1:]:
        total = total + share
    half = mine_ref.shape[0]
    halves = []
    for at in (0, half):
        mixed = None
        for s in range(parts):
            term = part_ref[s, :rows, at : at + half].astype(F32) * shares[s]
            mixed = term if mixed is None else mixed + term
        halves.append((mixed / total).astype(BF16))
    first = core_ref[0] == 0
    mine = jnp.where(first, halves[0], halves[1])
    other = jnp.where(first, halves[1], halves[0])
    projected = dot(mine, mine_ref[...]) + dot(other, other_ref[...])
    out_ref[...] = projected.astype(BF16).reshape(out_ref.shape)


def merge_and_project(core, parts, mine, other, chips):
    rows = parts.shape[1] - STATS
    return pl.pallas_call(
        merge_kernel,
        in_specs=[pl.BlockSpec(memory_space=pltpu.SMEM)] + in_vmem(3),
        out_specs=in_vmem(1)[0],
        out_shape=vmem_out((chips, rows // chips, mine.shape[1])),
        name="merge_and_project",
    )(core, *held_in_vmem(parts, mine, other))


def finish_kernel(part_ref, residual_ref, out_gain_ref, *rest):
    summed = jnp.sum(part_ref[...].astype(F32), axis=0)
    residual = (residual_ref[...].astype(F32) + scaled(summed, out_gain_ref[...])).astype(BF16)
    if len(rest) == 1:
        rest[0][...] = residual
    else:
        rest[1][...] = residual
        rest[2][...] = scaled(residual.astype(F32), rest[0][...]).astype(BF16)


def finish(parts, residual, out_gain, next_gain=None):
    shape = jax.ShapeDtypeStruct(residual.shape, BF16)
    extra = () if next_gain is None else (next_gain,)
    return pl.pallas_call(
        finish_kernel,
        in_specs=in_vmem(3 + len(extra)),
        out_specs=in_vmem(1 + len(extra)),
        out_shape=[shape] * (1 + len(extra)),
        name="finish",
    )(*held_in_vmem(parts, residual, out_gain, *extra))


def exchange(value, axis):
    return lax.all_to_all(value, axis, split_axis=0, concat_axis=0, tiled=True)


def to_all(value, axis, peers):
    return exchange(jnp.broadcast_to(value, (peers, *value.shape)), axis)


def swap(value):
    return lax.ppermute(value, "core", [(0, 1), (1, 0)])


def body(
    target,
    source,
    source_gain,
    query_gain,
    out_gain,
    query_weight,
    key_weight,
    value_weight,
    out_weight,
):
    quarters = lax.axis_size("quarter")
    chips = quarters * lax.axis_size("kv")
    stages = lax.axis_size("sp")
    core = lax.axis_index("core").astype(jnp.int32).reshape(1)
    width = key_weight.shape[2]

    columns = source_columns(source, source_gain[None], key_weight, value_weight, quarters)
    columns = columns.reshape(quarters * 2, LAYERS * width, -1)
    held = exchange(columns, GROUP)
    normed = first_norm(target, query_gain[:1])
    near = []
    for layer in range(LAYERS):
        block = held[:, layer * width : (layer + 1) * width].reshape(HD, -1)
        near.append(lax.all_gather(block, "sp", axis=0))
    far = [swap(part) for part in near]
    query_other = swap(query_weight)
    out_other = swap(out_weight)

    residual = target
    for layer in range(LAYERS):
        rows = to_all(normed, CHIPS, chips)
        mine = project_queries(core, rows, query_weight[layer], query_other[layer])
        queries = to_all(mine, "quarter", quarters)
        parts = attend(core, queries, near[layer], far[layer])
        parts = exchange(parts, "quarter")
        projected = merge_and_project(core, parts, out_weight[layer], out_other[layer], chips)
        arrived = exchange(projected, CHIPS)
        if layer + 1 < LAYERS:
            residual, normed = finish(
                arrived, residual, out_gain[layer : layer + 1], query_gain[layer + 1 : layer + 2]
            )
        else:
            (residual,) = finish(arrived, residual, out_gain[layer : layer + 1])
    return residual


def solution(mesh):
    groups, stages, devices = mesh.devices.shape
    own = Mesh(
        mesh.devices.reshape(groups, stages, KVH, devices // (2 * KVH), 2),
        ("grp", "sp", "kv", "quarter", "core"),
    )
    every = ("grp", "sp", "kv", "quarter", "core")
    tp = ("kv", "quarter", "core")
    in_specs = (
        P(every, None),
        P(("grp", "sp"), None),
        P(),
        P(),
        P(),
        P(None, None, tp),
        P(None, None, tp),
        P(None, None, tp),
        P(None, tp, None),
    )
    return jax.shard_map(body, mesh=own, in_specs=in_specs, out_specs=P(every, None), check_vma=False)
```

```python
import functools

import jax
import jax.numpy as jnp
from jax import lax
from jax.experimental import pallas as pl
from jax.experimental.pallas import tpu as pltpu
from jax.sharding import Mesh
from jax.sharding import PartitionSpec as P


HD = 256
KVH = 2
LAYERS = 2
EPSILON = 1e-06
STATS = 16

CHIPS = ("kv", "quarter")
GROUP = ("quarter", "core")
COPIES = (4, 0)
BF16 = jnp.bfloat16
F32 = jnp.float32


def dot(a, b, contract=((1,), (0,))):
    return lax.dot_general(a, b, (contract, ((), ())), preferred_element_type=F32)


def scaled(values, gain):
    inverse = lax.rsqrt(jnp.mean(values * values, axis=-1, keepdims=True) + EPSILON)
    return values * inverse * gain


def held_in_vmem(*arrays):
    return [pltpu.with_memory_space_constraint(a, pltpu.VMEM) for a in arrays]


def vmem_out(shape):
    return pltpu.VMEM(tuple(shape), BF16)


def in_vmem(count):
    return [pl.BlockSpec(memory_space=pltpu.VMEM)] * count


def source_kernel(source_ref, gain_ref, key_ref, value_ref, out_ref, weight_ref):
    width = key_ref.shape[1]

    @pl.when(pl.program_id(0) == 0)
    def _():
        for layer in range(LAYERS):
            weight_ref[layer * width : (layer + 1) * width, :] = key_ref[layer]
            weight_ref[(LAYERS + layer) * width : (LAYERS + layer + 1) * width, :] = value_ref[layer]

    normed = scaled(source_ref[...].astype(F32), gain_ref[...]).astype(BF16)
    columns = dot(weight_ref[...], normed, ((1,), (1,))).astype(BF16)
    out_ref[...] = columns.reshape(out_ref.shape)


def source_columns(source, gain, key_weight, value_weight, quarters):
    rows, features = source.shape
    key_weight = jnp.swapaxes(key_weight, 1, 2)
    value_weight = jnp.swapaxes(value_weight, 1, 2)
    width = key_weight.shape[1]
    block = rows // quarters
    return pl.pallas_call(
        source_kernel,
        grid=(quarters,),
        in_specs=[
            pl.BlockSpec((block, features), lambda i: (i, 0)),
            pl.BlockSpec((1, features), lambda i: (0, 0)),
            pl.BlockSpec(key_weight.shape, lambda i: (0, 0, 0)),
            pl.BlockSpec(value_weight.shape, lambda i: (0, 0, 0)),
        ],
        out_specs=pl.BlockSpec((1, 2, LAYERS * width, block), lambda i: (i, 0, 0, 0)),
        out_shape=jax.ShapeDtypeStruct((quarters, 2, LAYERS * width, block), BF16),
        scratch_shapes=[pltpu.VMEM((2 * LAYERS * width, features), BF16)],
        compiler_params=pltpu.CompilerParams(vmem_limit_bytes=12288 * 1024),
        name="source_columns",
    )(*[pltpu.with_memory_space_constraint(a, pltpu.HBM) for a in (source, gain, key_weight, value_weight)])


def norm_kernel(rows_ref, gain_ref, out_ref):
    normed = scaled(rows_ref[...].astype(F32), gain_ref[:1, :]).astype(BF16)
    for peer in range(out_ref.shape[0]):
        out_ref[peer] = normed


def first_norm(rows, gain, chips):
    return pl.pallas_call(
        norm_kernel,
        in_specs=in_vmem(2),
        out_specs=in_vmem(1)[0],
        out_shape=vmem_out((chips, *rows.shape)),
        compiler_params=pltpu.CompilerParams(vmem_limit_bytes=4096 * 1024),
        name="first_norm",
    )(*held_in_vmem(rows, gain))


def query_kernel(layer, core_ref, rows_ref, mine_ref, other_ref, out_ref):
    chips, block, features = rows_ref.shape
    rows = rows_ref[...].reshape(chips * block, features)
    mine = dot(rows, mine_ref[layer]).astype(BF16)
    other = dot(rows, other_ref[layer]).astype(BF16)
    first = core_ref[0] == 0
    width = mine.shape[1]
    low = jnp.where(first, mine, other)
    high = jnp.where(first, other, mine)
    for peer in range(out_ref.shape[0]):
        out_ref[peer, :, :width] = low
        out_ref[peer, :, width:] = high


def project_queries(layer, core, rows, mine, other, copies):
    chips, block, _ = rows.shape
    return pl.pallas_call(
        functools.partial(query_kernel, layer),
        in_specs=[pl.BlockSpec(memory_space=pltpu.SMEM)] + in_vmem(3),
        out_specs=in_vmem(1)[0],
        out_shape=vmem_out((copies, chips * block, 2 * mine.shape[2])),
        compiler_params=pltpu.CompilerParams(vmem_limit_bytes=8192 * 1024),
        name="project_queries",
    )(core, *held_in_vmem(rows, mine, other))


def attend_kernel(pieces, core_ref, query_ref, *refs):
    mine_refs, other_refs = refs[:pieces], refs[pieces : 2 * pieces]
    out_ref, score_ref = refs[2 * pieces :]
    heads, rows, width = query_ref.shape
    queries = query_ref[...].reshape(heads * rows, width)
    scale = width ** (-0.5)

    def pairs(piece_refs):
        for ref in piece_refs:
            for b in range(0, ref.shape[0], 2):
                yield jnp.concatenate([ref[b], ref[b + 1]], axis=1)

    def work(key_refs, value_refs):
        peak, at, spans = None, 0, []
        for keys in pairs(key_refs):
            scores = dot(queries, keys) * scale
            spans.append(slice(at, at + keys.shape[1]))
            score_ref[:, spans[-1]] = scores
            at += keys.shape[1]
            top = jnp.max(scores, axis=1, keepdims=True)
            peak = top if peak is None else jnp.maximum(peak, top)
        total, mixed = None, None
        for span, values in zip(spans, pairs(value_refs)):
            weights = jnp.exp(score_ref[:, span] - peak)
            part = jnp.sum(weights, axis=1, keepdims=True)
            share = dot(weights.astype(BF16), values, ((1,), (1,)))
            total = part if total is None else total + part
            mixed = share if mixed is None else mixed + share
        out_ref[:, :rows, :] = (mixed / total).astype(BF16).reshape(heads, rows, width)
        level = peak + jnp.log(total)
        high = level.astype(BF16).astype(F32)
        low = level - high
        for h in range(heads):
            for part, at in ((high, 0), (low, rows)):
                column = jnp.broadcast_to(part[h * rows : (h + 1) * rows], (rows, rows))
                out_ref[h, rows:, at : at + rows] = column.T[:STATS].astype(BF16)

    @pl.when(core_ref[0] == 0)
    def _():
        work(mine_refs, other_refs)

    @pl.when(core_ref[0] != 0)
    def _():
        work(other_refs, mine_refs)


def attend(core, queries, mine, other):
    heads, rows, width = queries.shape
    span = sum(piece.shape[0] * piece.shape[2] for piece in mine)
    return pl.pallas_call(
        functools.partial(attend_kernel, len(mine)),
        in_specs=[pl.BlockSpec(memory_space=pltpu.SMEM)] + in_vmem(1 + 2 * len(mine)),
        out_specs=in_vmem(1)[0],
        out_shape=vmem_out((heads, rows + STATS, width)),
        scratch_shapes=[pltpu.VMEM((heads * rows, span), F32)],
        compiler_params=pltpu.CompilerParams(vmem_limit_bytes=20480 * 1024),
        name="attend",
    )(core, *held_in_vmem(queries, *mine, *other))


def join_kernel(*refs):
    at = 0
    for ref in refs[:-1]:
        refs[-1][at : at + ref.shape[0]] = ref[...]
        at += ref.shape[0]


def join(*pieces):
    count = sum(piece.shape[0] for piece in pieces)
    return pl.pallas_call(
        join_kernel,
        in_specs=in_vmem(len(pieces)),
        out_specs=in_vmem(1)[0],
        out_shape=vmem_out((count, *pieces[0].shape[1:])),
        compiler_params=pltpu.CompilerParams(vmem_limit_bytes=4096 * 1024),
        name="join",
    )(*held_in_vmem(*pieces))


def merge_kernel(layer, core_ref, part_ref, mine_ref, other_ref, out_ref):
    parts, extended, _ = part_ref.shape
    rows = extended - STATS
    levels = []
    for s in range(parts):
        stats = part_ref[s, rows:, :].astype(F32)
        line = stats[:1, :rows] + stats[:1, rows:]
        levels.append(jnp.broadcast_to(line, (rows, rows)).T)
    peak = levels[0]
    for level in levels[1:]:
        peak = jnp.maximum(peak, level)
    shares = [jnp.exp(level - peak) for level in levels]
    total = shares[0]
    for share in shares[1:]:
        total = total + share
    half = mine_ref.shape[1]
    halves = []
    for at in (0, half):
        mixed = None
        for s in range(parts):
            term = part_ref[s, :rows, at : at + half].astype(F32) * shares[s]
            mixed = term if mixed is None else mixed + term
        halves.append((mixed / total).astype(BF16))
    first = core_ref[0] == 0
    mine = jnp.where(first, halves[0], halves[1])
    other = jnp.where(first, halves[1], halves[0])
    projected = dot(mine, mine_ref[layer]) + dot(other, other_ref[layer])
    out_ref[...] = projected.astype(BF16).reshape(out_ref.shape)


def merge_and_project(layer, core, parts, mine, other, chips):
    rows = parts.shape[1] - STATS
    return pl.pallas_call(
        functools.partial(merge_kernel, layer),
        in_specs=[pl.BlockSpec(memory_space=pltpu.SMEM)] + in_vmem(3),
        out_specs=in_vmem(1)[0],
        out_shape=vmem_out((chips, rows // chips, mine.shape[2])),
        compiler_params=pltpu.CompilerParams(vmem_limit_bytes=8192 * 1024),
        name="merge_and_project",
    )(core, *held_in_vmem(parts, mine, other))


def finish_kernel(layer, part_ref, residual_ref, out_gain_ref, query_gain_ref, *out_refs):
    summed = jnp.sum(part_ref[...].astype(F32), axis=0)
    change = scaled(summed, out_gain_ref[layer : layer + 1, :])
    residual = (residual_ref[...].astype(F32) + change).astype(BF16)
    out_refs[0][...] = residual
    if layer + 1 < LAYERS:
        normed = scaled(residual.astype(F32), query_gain_ref[layer + 1 : layer + 2, :]).astype(BF16)
        for peer in range(out_refs[1].shape[0]):
            out_refs[1][peer] = normed


def finish(layer, parts, residual, out_gain, query_gain):
    shapes = [residual.shape]
    if layer + 1 < LAYERS:
        shapes.append(parts.shape)
    return pl.pallas_call(
        functools.partial(finish_kernel, layer),
        in_specs=in_vmem(4),
        out_specs=in_vmem(len(shapes)),
        out_shape=[vmem_out(shape) for shape in shapes],
        compiler_params=pltpu.CompilerParams(vmem_limit_bytes=4096 * 1024),
        name="finish",
    )(*held_in_vmem(parts, residual, out_gain, query_gain))


def exchange(value, axis):
    return lax.all_to_all(value, axis, split_axis=0, concat_axis=0, tiled=True)


def shifted(value, distance, size):
    return lax.ppermute(value, "sp", [(z, (z + distance) % size) for z in range(size)])


def swap(value):
    return lax.ppermute(value, "core", [(0, 1), (1, 0)])


def after(value, *others):
    return lax.optimization_barrier((value, *others))[0]


def stride_step(block, stride, size):
    sent = [shifted(block, distance, size) for distance in (stride, -stride, 2 * stride)]
    return sent[0], block, sent[1], sent[2]


def near_step(own, size):
    return (
        shifted(own, 1, size),
        shifted(own, -1, size),
        shifted(own[:2], 2, size),
        shifted(own[1:3], -2, size),
    )


def layers(
    target,
    source,
    source_gain,
    query_gain,
    out_gain,
    query_weight,
    key_weight,
    value_weight,
    out_weight,
):
    quarters = lax.axis_size("quarter")
    chips = quarters * lax.axis_size("kv")
    stages = lax.axis_size("sp")
    core = lax.axis_index("core").astype(jnp.int32).reshape(1)
    width = key_weight.shape[2]

    columns = source_columns(source, source_gain[None], key_weight, value_weight, quarters)
    columns = columns.reshape(quarters * 2, LAYERS * width, -1)
    held = exchange(columns, GROUP)
    blocks = [
        held[:, layer * width : (layer + 1) * width].reshape(1, HD, -1) for layer in range(LAYERS)
    ]
    near, far = [], []
    pieces = stride_step(blocks[0], stages // 4, stages)
    own = join(*pieces)
    pieces = near_step(own, stages)
    far_own = swap(own)
    rest = join(*pieces)
    far_rest = swap(rest)
    near.append((own, rest))
    far.append((far_own, far_rest))
    normed = after(first_norm(target, query_gain, chips), held)
    query_other = swap(query_weight)
    out_other = swap(out_weight)

    residual = target
    for layer in range(LAYERS):
        rows = exchange(normed, CHIPS)
        mine = project_queries(layer, core, rows, query_weight, query_other, COPIES[layer] or 1)
        if layer == 0:
            pieces = stride_step(after(blocks[1], mine), stages // 4, stages)
        if COPIES[layer]:
            queries = exchange(mine, "quarter")
        else:
            queries = lax.all_gather(mine[0], "quarter", axis=0)
        parts = attend(core, queries, near[layer], far[layer])
        if layer == 0:
            own = join(*after(pieces, parts))
            pieces = near_step(own, stages)
        parts = exchange(parts, "quarter")
        projected = merge_and_project(layer, core, parts, out_weight, out_other, chips)
        arrived = exchange(projected, CHIPS)
        if layer == 0:
            whole = join(own, *after(pieces, projected))
            far.append((swap(whole),))
            near.append((whole,))
        done = finish(layer, arrived, residual, out_gain, query_gain)
        residual = done[0]
        normed = done[-1]
    return residual


def solution(mesh):
    groups, stages, devices = mesh.devices.shape
    own = Mesh(
        mesh.devices.reshape(groups, stages, KVH, devices // (2 * KVH), 2),
        ("grp", "sp", "kv", "quarter", "core"),
    )
    every = ("grp", "sp", "kv", "quarter", "core")
    tp = ("kv", "quarter", "core")
    in_specs = (
        P(every, None),
        P(("grp", "sp"), None),
        P(),
        P(),
        P(),
        P(None, None, tp),
        P(None, None, tp),
        P(None, None, tp),
        P(None, tp, None),
    )
    return jax.shard_map(layers, mesh=own, in_specs=in_specs, out_specs=P(every, None), check_vma=False)
```

```python
import functools

import jax
import jax.numpy as jnp
from jax import lax
from jax.experimental import pallas as pl
from jax.experimental.pallas import tpu as pltpu
from jax.sharding import Mesh
from jax.sharding import PartitionSpec as P


HD = 256
KVH = 2
LAYERS = 2
EPSILON = 1e-06
STATS = 16

CHIPS = ("kv", "quarter")
GROUP = ("quarter", "core")
BF16 = jnp.bfloat16
F32 = jnp.float32


def dot(a, b, contract=((1,), (0,))):
    return lax.dot_general(a, b, (contract, ((), ())), preferred_element_type=F32)


def scaled(values, gain):
    inverse = lax.rsqrt(jnp.mean(values * values, axis=-1, keepdims=True) + EPSILON)
    return values * inverse * gain


def held_in_vmem(*arrays):
    return [pltpu.with_memory_space_constraint(a, pltpu.VMEM) for a in arrays]


def vmem_out(shape):
    return pltpu.VMEM(tuple(shape), BF16)


def in_vmem(count):
    return [pl.BlockSpec(memory_space=pltpu.VMEM)] * count


def source_kernel(source_ref, gain_ref, key_ref, value_ref, out_ref, weight_ref):
    width = key_ref.shape[1]

    @pl.when(pl.program_id(0) == 0)
    def _():
        for layer in range(LAYERS):
            weight_ref[layer * width : (layer + 1) * width, :] = key_ref[layer]
            weight_ref[(LAYERS + layer) * width : (LAYERS + layer + 1) * width, :] = value_ref[layer]

    normed = scaled(source_ref[...].astype(F32), gain_ref[...]).astype(BF16)
    columns = dot(weight_ref[...], normed, ((1,), (1,))).astype(BF16)
    out_ref[...] = columns.reshape(out_ref.shape)


def source_columns(source, gain, key_weight, value_weight, quarters):
    rows, features = source.shape
    key_weight = jnp.swapaxes(key_weight, 1, 2)
    value_weight = jnp.swapaxes(value_weight, 1, 2)
    width = key_weight.shape[1]
    block = rows // quarters
    return pl.pallas_call(
        source_kernel,
        grid=(quarters,),
        in_specs=[
            pl.BlockSpec((block, features), lambda i: (i, 0)),
            pl.BlockSpec((1, features), lambda i: (0, 0)),
            pl.BlockSpec(key_weight.shape, lambda i: (0, 0, 0)),
            pl.BlockSpec(value_weight.shape, lambda i: (0, 0, 0)),
        ],
        out_specs=pl.BlockSpec((1, 2, LAYERS * width, block), lambda i: (i, 0, 0, 0)),
        out_shape=jax.ShapeDtypeStruct((quarters, 2, LAYERS * width, block), BF16),
        scratch_shapes=[pltpu.VMEM((2 * LAYERS * width, features), BF16)],
        compiler_params=pltpu.CompilerParams(vmem_limit_bytes=12288 * 1024),
        name="source_columns",
    )(*[pltpu.with_memory_space_constraint(a, pltpu.HBM) for a in (source, gain, key_weight, value_weight)])


def norm_kernel(rows_ref, gain_ref, out_ref):
    normed = scaled(rows_ref[...].astype(F32), gain_ref[:1, :]).astype(BF16)
    for peer in range(out_ref.shape[0]):
        out_ref[peer] = normed


def first_norm(rows, gain, chips):
    return pl.pallas_call(
        norm_kernel,
        in_specs=in_vmem(2),
        out_specs=in_vmem(1)[0],
        out_shape=pltpu.HBM((chips, *rows.shape), BF16),
        compiler_params=pltpu.CompilerParams(vmem_limit_bytes=4096 * 1024),
        name="first_norm",
    )(*held_in_vmem(rows, gain))


def query_kernel(layer, core_ref, rows_ref, mine_ref, other_ref, out_ref):
    chips, block, features = rows_ref.shape
    rows = rows_ref[...].reshape(chips * block, features)
    mine = dot(rows, mine_ref[layer]).astype(BF16)
    other = dot(rows, other_ref[layer]).astype(BF16)
    first = core_ref[0] == 0
    width = mine.shape[1]
    low = jnp.where(first, mine, other)
    high = jnp.where(first, other, mine)
    for peer in range(out_ref.shape[0]):
        out_ref[peer, :, :width] = low
        out_ref[peer, :, width:] = high


def project_queries(layer, core, rows, mine, other, copies):
    chips, block, _ = rows.shape
    return pl.pallas_call(
        functools.partial(query_kernel, layer),
        in_specs=[pl.BlockSpec(memory_space=pltpu.SMEM)] + in_vmem(3),
        out_specs=in_vmem(1)[0],
        out_shape=pltpu.HBM((copies, chips * block, 2 * mine.shape[2]), BF16),
        compiler_params=pltpu.CompilerParams(vmem_limit_bytes=8192 * 1024),
        name="project_queries",
    )(core, *held_in_vmem(rows, mine, other))


def attend_kernel(pieces, core_ref, query_ref, *refs):
    mine_refs, other_refs = refs[:pieces], refs[pieces : 2 * pieces]
    out_ref, score_ref = refs[2 * pieces :]
    heads, rows, width = query_ref.shape
    queries = query_ref[...].reshape(heads * rows, width)
    scale = width ** (-0.5)

    def pairs(piece_refs):
        for ref in piece_refs:
            for b in range(0, ref.shape[0], 2):
                yield jnp.concatenate([ref[b], ref[b + 1]], axis=1)

    def work(key_refs, value_refs):
        peak, at, spans = None, 0, []
        for keys in pairs(key_refs):
            scores = dot(queries, keys) * scale
            spans.append(slice(at, at + keys.shape[1]))
            score_ref[:, spans[-1]] = scores
            at += keys.shape[1]
            top = jnp.max(scores, axis=1, keepdims=True)
            peak = top if peak is None else jnp.maximum(peak, top)
        total, mixed = None, None
        for span, values in zip(spans, pairs(value_refs)):
            weights = jnp.exp(score_ref[:, span] - peak)
            part = jnp.sum(weights, axis=1, keepdims=True)
            share = dot(weights.astype(BF16), values, ((1,), (1,)))
            total = part if total is None else total + part
            mixed = share if mixed is None else mixed + share
        out_ref[:, :rows, :] = (mixed / total).astype(BF16).reshape(heads, rows, width)
        level = peak + jnp.log(total)
        high = level.astype(BF16).astype(F32)
        low = level - high
        for h in range(heads):
            for part, at in ((high, 0), (low, rows)):
                column = jnp.broadcast_to(part[h * rows : (h + 1) * rows], (rows, rows))
                out_ref[h, rows:, at : at + rows] = column.T[:STATS].astype(BF16)

    @pl.when(core_ref[0] == 0)
    def _():
        work(mine_refs, other_refs)

    @pl.when(core_ref[0] != 0)
    def _():
        work(other_refs, mine_refs)


def attend(core, queries, mine, other):
    heads, rows, width = queries.shape
    span = sum(piece.shape[0] * piece.shape[2] for piece in mine)
    return pl.pallas_call(
        functools.partial(attend_kernel, len(mine)),
        in_specs=[pl.BlockSpec(memory_space=pltpu.SMEM)] + in_vmem(1 + 2 * len(mine)),
        out_specs=in_vmem(1)[0],
        out_shape=pltpu.HBM((heads, rows + STATS, width), BF16),
        scratch_shapes=[pltpu.VMEM((heads * rows, span), F32)],
        compiler_params=pltpu.CompilerParams(vmem_limit_bytes=14336 * 1024),
        name="attend",
    )(core, *held_in_vmem(queries, *mine, *other))


def join_kernel(*refs):
    at = 0
    for ref in refs[:-1]:
        refs[-1][at : at + ref.shape[0]] = ref[...]
        at += ref.shape[0]


def join(*pieces):
    count = sum(piece.shape[0] for piece in pieces)
    return pl.pallas_call(
        join_kernel,
        in_specs=in_vmem(len(pieces)),
        out_specs=in_vmem(1)[0],
        out_shape=vmem_out((count, *pieces[0].shape[1:])),
        compiler_params=pltpu.CompilerParams(vmem_limit_bytes=4096 * 1024),
        name="join",
    )(*held_in_vmem(*pieces))


def merge_kernel(layer, core_ref, part_ref, mine_ref, other_ref, out_ref):
    parts, extended, _ = part_ref.shape
    rows = extended - STATS
    levels = []
    for s in range(parts):
        stats = part_ref[s, rows:, :].astype(F32)
        line = stats[:1, :rows] + stats[:1, rows:]
        levels.append(jnp.broadcast_to(line, (rows, rows)).T)
    peak = levels[0]
    for level in levels[1:]:
        peak = jnp.maximum(peak, level)
    shares = [jnp.exp(level - peak) for level in levels]
    total = shares[0]
    for share in shares[1:]:
        total = total + share
    half = mine_ref.shape[1]
    halves = []
    for at in (0, half):
        mixed = None
        for s in range(parts):
            term = part_ref[s, :rows, at : at + half].astype(F32) * shares[s]
            mixed = term if mixed is None else mixed + term
        halves.append((mixed / total).astype(BF16))
    first = core_ref[0] == 0
    mine = jnp.where(first, halves[0], halves[1])
    other = jnp.where(first, halves[1], halves[0])
    projected = dot(mine, mine_ref[layer]) + dot(other, other_ref[layer])
    out_ref[...] = projected.astype(BF16).reshape(out_ref.shape)


def merge_and_project(layer, core, parts, mine, other, chips):
    rows = parts.shape[1] - STATS
    return pl.pallas_call(
        functools.partial(merge_kernel, layer),
        in_specs=[pl.BlockSpec(memory_space=pltpu.SMEM)] + in_vmem(3),
        out_specs=in_vmem(1)[0],
        out_shape=pltpu.HBM((chips, rows // chips, mine.shape[2]), BF16),
        compiler_params=pltpu.CompilerParams(vmem_limit_bytes=8192 * 1024),
        name="merge_and_project",
    )(core, *held_in_vmem(parts, mine, other))


def finish_kernel(layer, part_ref, residual_ref, out_gain_ref, query_gain_ref, *out_refs):
    summed = jnp.sum(part_ref[...].astype(F32), axis=0)
    change = scaled(summed, out_gain_ref[layer : layer + 1, :])
    residual = (residual_ref[...].astype(F32) + change).astype(BF16)
    out_refs[0][...] = residual
    if layer + 1 < LAYERS:
        normed = scaled(residual.astype(F32), query_gain_ref[layer + 1 : layer + 2, :]).astype(BF16)
        for peer in range(out_refs[1].shape[0]):
            out_refs[1][peer] = normed


def finish(layer, parts, residual, out_gain, query_gain):
    shapes = [residual.shape]
    if layer + 1 < LAYERS:
        shapes.append(parts.shape)
    return pl.pallas_call(
        functools.partial(finish_kernel, layer),
        in_specs=in_vmem(4),
        out_specs=in_vmem(len(shapes)),
        out_shape=[pltpu.HBM(shape, BF16) for shape in shapes],
        compiler_params=pltpu.CompilerParams(vmem_limit_bytes=4096 * 1024),
        name="finish",
    )(*held_in_vmem(parts, residual, out_gain, query_gain))


def exchange(value, axis):
    return lax.all_to_all(value, axis, split_axis=0, concat_axis=0, tiled=True)


def shifted(value, distance, size):
    return lax.ppermute(value, "sp", [(z, (z + distance) % size) for z in range(size)])


def swap(value):
    return lax.ppermute(value, "core", [(0, 1), (1, 0)])


def after(value, *others):
    return lax.optimization_barrier((value, *others))[0]


def stride_step(block, stride, size):
    sent = [shifted(block, distance, size) for distance in (stride, -stride, 2 * stride)]
    return sent[0], block, sent[1], sent[2]


def near_step(own, size):
    return (
        shifted(own, 1, size),
        shifted(own, -1, size),
        shifted(own[:2], 2, size),
        shifted(own[1:3], -2, size),
    )


def layers(
    target,
    source,
    source_gain,
    query_gain,
    out_gain,
    query_weight,
    key_weight,
    value_weight,
    out_weight,
):
    quarters = lax.axis_size("quarter")
    chips = quarters * lax.axis_size("kv")
    stages = lax.axis_size("sp")
    core = lax.axis_index("core").astype(jnp.int32).reshape(1)
    width = key_weight.shape[2]

    columns = source_columns(source, source_gain[None], key_weight, value_weight, quarters)
    columns = columns.reshape(quarters * 2, LAYERS * width, -1)
    held = exchange(columns, GROUP)
    blocks = [
        held[:, layer * width : (layer + 1) * width].reshape(1, HD, -1) for layer in range(LAYERS)
    ]
    near, far = [], []
    pieces = stride_step(blocks[0], stages // 4, stages)
    own = join(*pieces)
    pieces = near_step(own, stages)
    far_own = swap(own)
    rest = join(*pieces)
    far_rest = swap(rest)
    near.append((own, rest))
    far.append((far_own, far_rest))
    normed = after(first_norm(target, query_gain, chips), held)
    query_other = swap(query_weight)
    out_other = swap(out_weight)

    residual = target
    for layer in range(LAYERS):
        rows = exchange(normed, CHIPS)
        mine = project_queries(layer, core, rows, query_weight, query_other, quarters)
        queries = exchange(mine, "quarter")
        parts = attend(core, queries, near[layer], far[layer])
        if layer == 0:
            pieces = stride_step(after(blocks[1], parts), stages // 4, stages)
        parts = exchange(parts, "quarter")
        projected = merge_and_project(layer, core, parts, out_weight, out_other, chips)
        if layer == 0:
            own = join(*after(pieces, projected))
            pieces = near_step(own, stages)
        arrived = exchange(projected, CHIPS)
        done = finish(layer, arrived, residual, out_gain, query_gain)
        residual = done[0]
        normed = done[-1]
        if layer == 0:
            whole = join(own, *after(pieces, normed))
            far.append((swap(whole),))
            near.append((whole,))
    return residual


def solution(mesh):
    groups, stages, devices = mesh.devices.shape
    own = Mesh(
        mesh.devices.reshape(groups, stages, KVH, devices // (2 * KVH), 2),
        ("grp", "sp", "kv", "quarter", "core"),
    )
    every = ("grp", "sp", "kv", "quarter", "core")
    tp = ("kv", "quarter", "core")
    in_specs = (
        P(every, None),
        P(("grp", "sp"), None),
        P(),
        P(),
        P(),
        P(None, None, tp),
        P(None, None, tp),
        P(None, None, tp),
        P(None, tp, None),
    )
    return jax.shard_map(layers, mesh=own, in_specs=in_specs, out_specs=P(every, None), check_vma=False)
```

```python
import functools

import jax
import jax.numpy as jnp
from jax import lax
from jax.experimental import pallas as pl
from jax.experimental.pallas import tpu as pltpu
from jax.sharding import Mesh
from jax.sharding import PartitionSpec as P


KVH = 2
LAYERS = 2
EPSILON = 1e-06
STATS = 16

CHIPS = ("kv", "quarter")
GROUP = ("quarter", "core")
BF16 = jnp.bfloat16
F32 = jnp.float32


def dot(a, b, contract=((1,), (0,))):
    return lax.dot_general(a, b, (contract, ((), ())), preferred_element_type=F32)


def scaled(values, gain):
    inverse = lax.rsqrt(jnp.mean(values * values, axis=-1, keepdims=True) + EPSILON)
    return values * inverse * gain


def held_in_vmem(*arrays):
    return [pltpu.with_memory_space_constraint(a, pltpu.VMEM) for a in arrays]


def vmem_out(shape):
    return pltpu.VMEM(tuple(shape), BF16)


def in_vmem(count):
    return [pl.BlockSpec(memory_space=pltpu.VMEM)] * count


def source_kernel(source_ref, gain_ref, key_ref, value_ref, out_ref, weight_ref):
    width = key_ref.shape[1]
    quarters = out_ref.shape[0]
    step = pl.program_id(0)

    @pl.when(step == 0)
    def _():
        for layer in range(LAYERS):
            weight_ref[layer * width : (layer + 1) * width, :] = key_ref[layer]
            weight_ref[(LAYERS + layer) * width : (LAYERS + layer + 1) * width, :] = value_ref[layer]

    normed = scaled(source_ref[...].astype(F32), gain_ref[...]).astype(BF16)
    columns = dot(weight_ref[...], normed, ((1,), (1,))).astype(BF16)
    for block in range(quarters):

        @pl.when(step == block)
        def _():
            half, at = block // 2, width * (1 + block % 2)
            for core in range(2):
                first = columns[2 * core * width : (2 * core + 1) * width]
                later = columns[(2 * core + 1) * width : (2 * core + 2) * width]
                out_ref[block, core, :width, :] = first
                for quarter in range(half, quarters, 2):
                    out_ref[quarter, core, at : at + width, :] = later


def source_columns(source, gain, key_weight, value_weight, quarters):
    rows, features = source.shape
    key_weight = jnp.swapaxes(key_weight, 1, 2)
    value_weight = jnp.swapaxes(value_weight, 1, 2)
    width = key_weight.shape[1]
    block = rows // quarters
    shape = (quarters, 2, 3 * width, block)
    operands = (source, gain, key_weight, value_weight)
    return pl.pallas_call(
        source_kernel,
        grid=(quarters,),
        in_specs=[
            pl.BlockSpec((block, features), lambda i: (i, 0)),
            pl.BlockSpec((1, features), lambda i: (0, 0)),
            pl.BlockSpec(key_weight.shape, lambda i: (0, 0, 0)),
            pl.BlockSpec(value_weight.shape, lambda i: (0, 0, 0)),
        ],
        out_specs=pl.BlockSpec(shape, lambda i: (0, 0, 0, 0)),
        out_shape=pltpu.HBM(shape, BF16),
        scratch_shapes=[pltpu.VMEM((2 * LAYERS * width, features), BF16)],
        compiler_params=pltpu.CompilerParams(vmem_limit_bytes=12288 * 1024),
        name="source_columns",
    )(*[pltpu.with_memory_space_constraint(a, pltpu.HBM) for a in operands])


def norm_kernel(rows_ref, gain_ref, out_ref):
    normed = scaled(rows_ref[...].astype(F32), gain_ref[:1, :]).astype(BF16)
    for peer in range(out_ref.shape[0]):
        out_ref[peer] = normed


def first_norm(rows, gain, chips):
    return pl.pallas_call(
        norm_kernel,
        in_specs=in_vmem(2),
        out_specs=in_vmem(1)[0],
        out_shape=pltpu.HBM((chips, *rows.shape), BF16),
        compiler_params=pltpu.CompilerParams(vmem_limit_bytes=4096 * 1024),
        name="first_norm",
    )(*held_in_vmem(rows, gain))


def query_kernel(layer, core_ref, rows_ref, mine_ref, other_ref, out_ref):
    chips, block, features = rows_ref.shape
    rows = rows_ref[...].reshape(chips * block, features)
    mine = dot(rows, mine_ref[layer]).astype(BF16)
    other = dot(rows, other_ref[layer]).astype(BF16)
    first = core_ref[0] == 0
    width = mine.shape[1]
    low = jnp.where(first, mine, other)
    high = jnp.where(first, other, mine)
    for peer in range(out_ref.shape[0]):
        out_ref[peer, :, :width] = low
        out_ref[peer, :, width:] = high


def project_queries(layer, core, rows, mine, other, copies, held):
    chips, block, _ = rows.shape
    return pl.pallas_call(
        functools.partial(query_kernel, layer),
        in_specs=[pl.BlockSpec(memory_space=pltpu.SMEM)] + in_vmem(3),
        out_specs=in_vmem(1)[0],
        out_shape=held((copies, chips * block, 2 * mine.shape[2]), BF16),
        compiler_params=pltpu.CompilerParams(vmem_limit_bytes=8192 * 1024),
        name="project_queries",
    )(core, pltpu.with_memory_space_constraint(rows, pltpu.HBM), *held_in_vmem(mine, other))


def attend_kernel(groups, pieces, core_ref, *refs):
    query_refs, refs = refs[:groups], refs[groups:]
    mine_refs, other_refs = refs[:pieces], refs[pieces : 2 * pieces]
    out_refs, score_ref = refs[2 * pieces : -1], refs[-1]
    heads, rows, width = query_refs[0].shape
    queries = [ref[...].reshape(heads * rows, width) for ref in query_refs]
    queries = queries[0] if groups == 1 else jnp.concatenate(queries, axis=0)
    scale = width ** (-0.5)

    def pairs(piece_refs):
        for ref in piece_refs:
            for b in range(0, ref.shape[0], 2):
                yield jnp.concatenate([ref[b], ref[b + 1]], axis=1)

    def work(key_refs, value_refs):
        peak, at, spans = None, 0, []
        for keys in pairs(key_refs):
            scores = dot(queries, keys) * scale
            spans.append(slice(at, at + keys.shape[1]))
            score_ref[:, spans[-1]] = scores
            at += keys.shape[1]
            top = jnp.max(scores, axis=1, keepdims=True)
            peak = top if peak is None else jnp.maximum(peak, top)
        total, mixed = None, None
        for span, values in zip(spans, pairs(value_refs)):
            weights = jnp.exp(score_ref[:, span] - peak)
            part = jnp.sum(weights, axis=1, keepdims=True)
            share = dot(weights.astype(BF16), values, ((1,), (1,)))
            total = part if total is None else total + part
            mixed = share if mixed is None else mixed + share
        attended = (mixed / total).astype(BF16)
        level = peak + jnp.log(total)
        high = level.astype(BF16).astype(F32)
        low = level - high
        for h in range(heads * groups):
            out_ref, own = out_refs[h // heads], slice(h * rows, (h + 1) * rows)
            out_ref[h % heads, :rows, :] = attended[own]
            for part, at in ((high, 0), (low, rows)):
                column = jnp.broadcast_to(part[own], (rows, rows))
                out_ref[h % heads, rows:, at : at + rows] = column.T[:STATS].astype(BF16)

    @pl.when(core_ref[0] == 0)
    def _():
        work(mine_refs, other_refs)

    @pl.when(core_ref[0] != 0)
    def _():
        work(other_refs, mine_refs)


def attend(core, queries, mine, other):
    heads, rows, width = queries[0].shape
    groups = len(queries)
    span = sum(piece.shape[0] * piece.shape[2] for piece in mine)
    return pl.pallas_call(
        functools.partial(attend_kernel, groups, len(mine)),
        in_specs=[pl.BlockSpec(memory_space=pltpu.SMEM)] + in_vmem(groups + 2 * len(mine)),
        out_specs=in_vmem(groups),
        out_shape=[vmem_out((heads, rows + STATS, width))] * groups,
        scratch_shapes=[pltpu.VMEM((groups * heads * rows, span), F32)],
        compiler_params=pltpu.CompilerParams(vmem_limit_bytes=16384 * 1024),
        name="attend",
    )(core, *held_in_vmem(*queries, *mine, *other))


def split_kernel(held_ref, first_ref, later_ref):
    devices, width, _ = held_ref.shape
    width //= 3
    for device in range(devices):
        columns = slice(device * width, (device + 1) * width)
        first_ref[0, columns, :] = held_ref[device, :width, :]
        for half in range(2):
            at = width * (1 + half)
            later_ref[half, columns, :] = held_ref[device, at : at + width, :]


def split(held):
    devices, width, block = held.shape
    column = devices * width // 3
    return pl.pallas_call(
        split_kernel,
        in_specs=in_vmem(1),
        out_specs=in_vmem(2),
        out_shape=[vmem_out((1, column, block)), pltpu.HBM((2, column, block), BF16)],
        compiler_params=pltpu.CompilerParams(vmem_limit_bytes=2048 * 1024),
        name="split",
    )(*held_in_vmem(held))


def four_kernel(*refs):
    pieces, (own_ref, low_ref, middle_ref) = refs[:4], refs[4:]
    for at, ref in enumerate(pieces):
        block = ref[0]
        own_ref[at] = block
        if at < 2:
            low_ref[at] = block
        if 1 <= at < 3:
            middle_ref[at - 1] = block


def join_four(*pieces):
    shape = pieces[0].shape[1:]
    return pl.pallas_call(
        four_kernel,
        in_specs=in_vmem(4),
        out_specs=in_vmem(3),
        out_shape=[vmem_out((count, *shape)) for count in (4, 2, 2)],
        compiler_params=pltpu.CompilerParams(vmem_limit_bytes=2048 * 1024),
        name="join_four",
    )(*held_in_vmem(*pieces))


def join_kernel(*refs):
    at = 0
    for ref in refs[:-1]:
        refs[-1][at : at + ref.shape[0]] = ref[...]
        at += ref.shape[0]


def join(*pieces):
    count = sum(piece.shape[0] for piece in pieces)
    return pl.pallas_call(
        join_kernel,
        in_specs=in_vmem(len(pieces)),
        out_specs=in_vmem(1)[0],
        out_shape=vmem_out((count, *pieces[0].shape[1:])),
        compiler_params=pltpu.CompilerParams(vmem_limit_bytes=4096 * 1024),
        name="join",
    )(*held_in_vmem(*pieces))


def merge_kernel(layer, core_ref, *refs):
    part_refs, (mine_ref, other_ref, out_ref) = refs[:-3], refs[-3:]
    parts = [ref.at[s] for ref in part_refs for s in range(ref.shape[0])]
    rows = parts[0].shape[0] - STATS
    levels = []
    for part in parts:
        stats = part[rows:, :].astype(F32)
        line = stats[:1, :rows] + stats[:1, rows:]
        levels.append(jnp.broadcast_to(line, (rows, rows)).T)
    peak = levels[0]
    for level in levels[1:]:
        peak = jnp.maximum(peak, level)
    shares = [jnp.exp(level - peak) for level in levels]
    total = shares[0]
    for share in shares[1:]:
        total = total + share
    half = mine_ref.shape[1]
    halves = []
    for at in (0, half):
        mixed = None
        for part, share in zip(parts, shares):
            term = part[:rows, at : at + half].astype(F32) * share
            mixed = term if mixed is None else mixed + term
        halves.append((mixed / total).astype(BF16))
    first = core_ref[0] == 0
    mine = jnp.where(first, halves[0], halves[1])
    other = jnp.where(first, halves[1], halves[0])
    projected = dot(mine, mine_ref[layer]) + dot(other, other_ref[layer])
    out_ref[...] = projected.astype(BF16).reshape(out_ref.shape)


def merge_and_project(layer, core, parts, mine, other, chips):
    rows = parts[0].shape[1] - STATS
    return pl.pallas_call(
        functools.partial(merge_kernel, layer),
        in_specs=[pl.BlockSpec(memory_space=pltpu.SMEM)] + in_vmem(len(parts) + 2),
        out_specs=in_vmem(1)[0],
        out_shape=vmem_out((chips, rows // chips, mine.shape[2])),
        compiler_params=pltpu.CompilerParams(vmem_limit_bytes=8192 * 1024),
        name="merge_and_project",
    )(core, *held_in_vmem(*parts, mine, other))


def finish_kernel(layer, part_ref, residual_ref, out_gain_ref, query_gain_ref, *out_refs):
    summed = jnp.sum(part_ref[...].astype(F32), axis=0)
    change = scaled(summed, out_gain_ref[layer : layer + 1, :])
    residual = (residual_ref[...].astype(F32) + change).astype(BF16)
    out_refs[0][...] = residual
    if layer + 1 < LAYERS:
        normed = scaled(residual.astype(F32), query_gain_ref[layer + 1 : layer + 2, :]).astype(BF16)
        for peer in range(out_refs[1].shape[0]):
            out_refs[1][peer] = normed


def finish(layer, parts, residual, out_gain, query_gain):
    shapes = [residual.shape]
    if layer + 1 < LAYERS:
        shapes.append(parts.shape)
    return pl.pallas_call(
        functools.partial(finish_kernel, layer),
        in_specs=in_vmem(4),
        out_specs=in_vmem(len(shapes)),
        out_shape=[jax.ShapeDtypeStruct(shapes[0], BF16)] + [pltpu.HBM(shape, BF16) for shape in shapes[1:]],
        compiler_params=pltpu.CompilerParams(vmem_limit_bytes=4096 * 1024),
        name="finish",
    )(*held_in_vmem(parts, residual, out_gain, query_gain))


def exchange(value, axis):
    return lax.all_to_all(value, axis, split_axis=0, concat_axis=0, tiled=True)


def shifted(value, distance, size):
    return lax.ppermute(value, "sp", [(z, (z + distance) % size) for z in range(size)])


def swap(value):
    return lax.ppermute(value, "core", [(0, 1), (1, 0)])


def beside(value, quarters):
    return lax.ppermute(value, "quarter", [(q, q ^ 1) for q in range(quarters)])


def after(value, *others):
    return lax.optimization_barrier((value, *others))[0]


def stride_step(block, stride, size):
    sent = [shifted(block, distance, size) for distance in (stride, -stride, 2 * stride)]
    return sent[0], block, sent[1], sent[2]


def near_step(own, low, middle, size):
    return (
        shifted(own, 1, size),
        shifted(own, -1, size),
        shifted(low, 2, size),
        shifted(middle, -2, size),
    )


def layers(
    target,
    source,
    source_gain,
    query_gain,
    out_gain,
    query_weight,
    key_weight,
    value_weight,
    out_weight,
):
    quarters = lax.axis_size("quarter")
    chips = quarters * lax.axis_size("kv")
    stages = lax.axis_size("sp")
    core = lax.axis_index("core").astype(jnp.int32).reshape(1)
    width = key_weight.shape[2]

    columns = source_columns(source, source_gain[None], key_weight, value_weight, quarters)
    columns = columns.reshape(quarters * 2, 3 * width, -1)
    held = exchange(columns, GROUP)
    first, later = split(held)
    pieces = stride_step(first, stages // 4, stages)
    own, low, middle = join_four(*pieces)
    pieces = near_step(own, low, middle, stages)
    near = join(own, *pieces)
    far = swap(near)
    normed = after(first_norm(target, query_gain, chips), held)
    query_other = swap(query_weight)
    out_other = swap(out_weight)
    near_later = lax.all_gather(after(later, near), "sp", axis=0, tiled=True)

    rows = exchange(normed, CHIPS)
    mine = project_queries(0, core, rows, query_weight, query_other, quarters, pltpu.HBM)
    queries = exchange(mine, "quarter")
    (parts,) = attend(core, [queries], [near], [far])
    parts, out_other = lax.optimization_barrier((parts, out_other))
    parts = exchange(parts, "quarter")
    projected = merge_and_project(0, core, [parts], out_weight, out_other, chips)
    arrived = exchange(projected, CHIPS)
    residual, normed = finish(0, arrived, target, out_gain, query_gain)

    rows = exchange(normed, CHIPS)
    far_later = swap(near_later)
    mine = project_queries(1, core, rows, query_weight, query_other, 1, pltpu.VMEM)
    theirs = beside(mine, quarters)
    kept, sent = attend(core, [mine, theirs], [near_later], [far_later])
    came = beside(sent, quarters)
    projected = merge_and_project(1, core, [kept, came], out_weight, out_other, chips)
    arrived = exchange(projected, CHIPS)
    (residual,) = finish(1, arrived, residual, out_gain, query_gain)
    return residual


def solution(mesh):
    groups, stages, devices = mesh.devices.shape
    own = Mesh(
        mesh.devices.reshape(groups, stages, KVH, devices // (2 * KVH), 2),
        ("grp", "sp", "kv", "quarter", "core"),
    )
    every = ("grp", "sp", "kv", "quarter", "core")
    tp = ("kv", "quarter", "core")
    in_specs = (
        P(every, None),
        P(("grp", "sp"), None),
        P(),
        P(),
        P(),
        P(None, None, tp),
        P(None, None, tp),
        P(None, None, tp),
        P(None, tp, None),
    )
    return jax.shard_map(layers, mesh=own, in_specs=in_specs, out_specs=P(every, None), check_vma=False)
```

```python
import functools

import jax
import jax.numpy as jnp
from jax import lax
from jax.experimental import pallas as pl
from jax.experimental.pallas import tpu as pltpu
from jax.sharding import Mesh
from jax.sharding import PartitionSpec as P


KVH = 2
LAYERS = 2
EPSILON = 1e-06
STATS = 16

CHIPS = ("kv", "quarter")
GROUP = ("quarter", "core")
STAGES = ("far", "near")
BF16 = jnp.bfloat16
F32 = jnp.float32


def dot(a, b, contract=((1,), (0,))):
    return lax.dot_general(a, b, (contract, ((), ())), preferred_element_type=F32)


def scaled(values, gain):
    inverse = lax.rsqrt(jnp.mean(values * values, axis=-1, keepdims=True) + EPSILON)
    return values * inverse * gain


def held_in_vmem(*arrays):
    return [pltpu.with_memory_space_constraint(a, pltpu.VMEM) for a in arrays]


def vmem_out(shape):
    return pltpu.VMEM(tuple(shape), BF16)


def in_vmem(count):
    return [pl.BlockSpec(memory_space=pltpu.VMEM)] * count


def source_kernel(source_ref, gain_ref, key_ref, value_ref, out_ref, weight_ref):
    width = key_ref.shape[1]
    quarters = out_ref.shape[0]
    step = pl.program_id(0)

    @pl.when(step == 0)
    def _():
        for layer in range(LAYERS):
            weight_ref[layer * width : (layer + 1) * width, :] = key_ref[layer]
            weight_ref[(LAYERS + layer) * width : (LAYERS + layer + 1) * width, :] = value_ref[layer]

    normed = scaled(source_ref[...].astype(F32), gain_ref[...]).astype(BF16)
    columns = dot(weight_ref[...], normed, ((1,), (1,))).astype(BF16)
    for block in range(quarters):

        @pl.when(step == block)
        def _():
            half, at = block // 2, width * (1 + block % 2)
            for core in range(2):
                first = columns[2 * core * width : (2 * core + 1) * width]
                later = columns[(2 * core + 1) * width : (2 * core + 2) * width]
                out_ref[block, core, :width, :] = first
                for quarter in range(half, quarters, 2):
                    out_ref[quarter, core, at : at + width, :] = later


def source_columns(source, gain, key_weight, value_weight, quarters):
    rows, features = source.shape
    key_weight = jnp.swapaxes(key_weight, 1, 2)
    value_weight = jnp.swapaxes(value_weight, 1, 2)
    width = key_weight.shape[1]
    block = rows // quarters
    shape = (quarters, 2, 3 * width, block)
    operands = (source, gain, key_weight, value_weight)
    return pl.pallas_call(
        source_kernel,
        grid=(quarters,),
        in_specs=[
            pl.BlockSpec((block, features), lambda i: (i, 0)),
            pl.BlockSpec((1, features), lambda i: (0, 0)),
            pl.BlockSpec(key_weight.shape, lambda i: (0, 0, 0)),
            pl.BlockSpec(value_weight.shape, lambda i: (0, 0, 0)),
        ],
        out_specs=pl.BlockSpec(shape, lambda i: (0, 0, 0, 0)),
        out_shape=pltpu.HBM(shape, BF16),
        scratch_shapes=[pltpu.VMEM((2 * LAYERS * width, features), BF16)],
        compiler_params=pltpu.CompilerParams(vmem_limit_bytes=12288 * 1024),
        name="source_columns",
    )(*[pltpu.with_memory_space_constraint(a, pltpu.HBM) for a in operands])


def norm_kernel(rows_ref, gain_ref, out_ref):
    normed = scaled(rows_ref[...].astype(F32), gain_ref[:1, :]).astype(BF16)
    for peer in range(out_ref.shape[0]):
        out_ref[peer] = normed


def first_norm(rows, gain, chips):
    return pl.pallas_call(
        norm_kernel,
        in_specs=in_vmem(2),
        out_specs=in_vmem(1)[0],
        out_shape=pltpu.HBM((chips, *rows.shape), BF16),
        compiler_params=pltpu.CompilerParams(vmem_limit_bytes=4096 * 1024),
        name="first_norm",
    )(*held_in_vmem(rows, gain))


def query_kernel(layer, core_ref, rows_ref, mine_ref, other_ref, out_ref):
    chips, block, features = rows_ref.shape
    rows = rows_ref[...].reshape(chips * block, features)
    mine = dot(rows, mine_ref[layer]).astype(BF16)
    other = dot(rows, other_ref[layer]).astype(BF16)
    first = core_ref[0] == 0
    width = mine.shape[1]
    low = jnp.where(first, mine, other)
    high = jnp.where(first, other, mine)
    for peer in range(out_ref.shape[0]):
        out_ref[peer, :, :width] = low
        out_ref[peer, :, width:] = high


def project_queries(layer, core, rows, mine, other, copies, held):
    chips, block, _ = rows.shape
    return pl.pallas_call(
        functools.partial(query_kernel, layer),
        in_specs=[pl.BlockSpec(memory_space=pltpu.SMEM)] + in_vmem(3),
        out_specs=in_vmem(1)[0],
        out_shape=held((copies, chips * block, 2 * mine.shape[2]), BF16),
        compiler_params=pltpu.CompilerParams(vmem_limit_bytes=8192 * 1024),
        name="project_queries",
    )(core, pltpu.with_memory_space_constraint(rows, pltpu.HBM), *held_in_vmem(mine, other))


def attend_kernel(groups, pieces, core_ref, *refs):
    query_refs, refs = refs[:groups], refs[groups:]
    mine_refs, other_refs = refs[:pieces], refs[pieces : 2 * pieces]
    out_refs, score_ref = refs[2 * pieces : -1], refs[-1]
    heads, rows, width = query_refs[0].shape
    queries = [ref[...].reshape(heads * rows, width) for ref in query_refs]
    queries = queries[0] if groups == 1 else jnp.concatenate(queries, axis=0)
    scale = width ** (-0.5)

    def pairs(piece_refs):
        for ref in piece_refs:
            for b in range(0, ref.shape[0], 2):
                yield jnp.concatenate([ref[b], ref[b + 1]], axis=1)

    def work(key_refs, value_refs):
        peak, at, spans = None, 0, []
        for keys in pairs(key_refs):
            scores = dot(queries, keys) * scale
            spans.append(slice(at, at + keys.shape[1]))
            score_ref[:, spans[-1]] = scores
            at += keys.shape[1]
            top = jnp.max(scores, axis=1, keepdims=True)
            peak = top if peak is None else jnp.maximum(peak, top)
        total, mixed = None, None
        for span, values in zip(spans, pairs(value_refs)):
            weights = jnp.exp(score_ref[:, span] - peak)
            part = jnp.sum(weights, axis=1, keepdims=True)
            share = dot(weights.astype(BF16), values, ((1,), (1,)))
            total = part if total is None else total + part
            mixed = share if mixed is None else mixed + share
        attended = (mixed / total).astype(BF16)
        level = peak + jnp.log(total)
        high = level.astype(BF16).astype(F32)
        low = level - high
        for h in range(heads * groups):
            out_ref, own = out_refs[h // heads], slice(h * rows, (h + 1) * rows)
            out_ref[h % heads, :rows, :] = attended[own]
            for part, at in ((high, 0), (low, rows)):
                column = jnp.broadcast_to(part[own], (rows, rows))
                out_ref[h % heads, rows:, at : at + rows] = column.T[:STATS].astype(BF16)

    @pl.when(core_ref[0] == 0)
    def _():
        work(mine_refs, other_refs)

    @pl.when(core_ref[0] != 0)
    def _():
        work(other_refs, mine_refs)


def attend(core, queries, mine, other):
    heads, rows, width = queries[0].shape
    groups = len(queries)
    span = sum(piece.shape[0] * piece.shape[2] for piece in mine)
    return pl.pallas_call(
        functools.partial(attend_kernel, groups, len(mine)),
        in_specs=[pl.BlockSpec(memory_space=pltpu.SMEM)] + in_vmem(groups + 2 * len(mine)),
        out_specs=in_vmem(groups),
        out_shape=[vmem_out((heads, rows + STATS, width))] * groups,
        scratch_shapes=[pltpu.VMEM((groups * heads * rows, span), F32)],
        compiler_params=pltpu.CompilerParams(vmem_limit_bytes=16384 * 1024),
        name="attend",
    )(core, *held_in_vmem(*queries), *[pltpu.with_memory_space_constraint(a, pltpu.HBM) for a in (*mine, *other)])


def split_kernel(held_ref, first_ref, later_ref):
    devices, width, _ = held_ref.shape
    width //= 3
    for device in range(devices):
        columns = slice(device * width, (device + 1) * width)
        for peer in range(first_ref.shape[0]):
            first_ref[peer, columns, :] = held_ref[device, :width, :]
        for half in range(2):
            at = width * (1 + half)
            later_ref[half, columns, :] = held_ref[device, at : at + width, :]


def split(held, copies):
    devices, width, block = held.shape
    column = devices * width // 3
    return pl.pallas_call(
        split_kernel,
        in_specs=in_vmem(1),
        out_specs=in_vmem(2),
        out_shape=[pltpu.HBM((count, column, block), BF16) for count in (copies, 2)],
        compiler_params=pltpu.CompilerParams(vmem_limit_bytes=2048 * 1024),
        name="split",
    )(*held_in_vmem(held))


def halves_kernel(own_ref, low_ref, high_ref):
    count = low_ref.shape[0]
    low_ref[...] = own_ref[:count]
    high_ref[...] = own_ref[count:]


def halves(own):
    shape = (own.shape[0] // 2, *own.shape[1:])
    return pl.pallas_call(
        halves_kernel,
        in_specs=in_vmem(1),
        out_specs=in_vmem(2),
        out_shape=[vmem_out(shape)] * 2,
        compiler_params=pltpu.CompilerParams(vmem_limit_bytes=2048 * 1024),
        name="halves",
    )(*held_in_vmem(own))


def join_kernel(*refs):
    at = 0
    for ref in refs[:-1]:
        refs[-1][at : at + ref.shape[0]] = ref[...]
        at += ref.shape[0]


def join(*pieces):
    count = sum(piece.shape[0] for piece in pieces)
    return pl.pallas_call(
        join_kernel,
        in_specs=in_vmem(len(pieces)),
        out_specs=in_vmem(1)[0],
        out_shape=pltpu.HBM((count, *pieces[0].shape[1:]), BF16),
        compiler_params=pltpu.CompilerParams(vmem_limit_bytes=4096 * 1024),
        name="join",
    )(*held_in_vmem(*pieces))


def merge_kernel(layer, core_ref, *refs):
    part_refs, (mine_ref, other_ref, out_ref) = refs[:-3], refs[-3:]
    parts = [ref.at[s] for ref in part_refs for s in range(ref.shape[0])]
    rows = parts[0].shape[0] - STATS
    levels = []
    for part in parts:
        stats = part[rows:, :].astype(F32)
        line = stats[:1, :rows] + stats[:1, rows:]
        levels.append(jnp.broadcast_to(line, (rows, rows)).T)
    peak = levels[0]
    for level in levels[1:]:
        peak = jnp.maximum(peak, level)
    shares = [jnp.exp(level - peak) for level in levels]
    total = shares[0]
    for share in shares[1:]:
        total = total + share
    half = mine_ref.shape[1]
    halves = []
    for at in (0, half):
        mixed = None
        for part, share in zip(parts, shares):
            term = part[:rows, at : at + half].astype(F32) * share
            mixed = term if mixed is None else mixed + term
        halves.append((mixed / total).astype(BF16))
    first = core_ref[0] == 0
    mine = jnp.where(first, halves[0], halves[1])
    other = jnp.where(first, halves[1], halves[0])
    projected = dot(mine, mine_ref[layer]) + dot(other, other_ref[layer])
    out_ref[...] = projected.astype(BF16).reshape(out_ref.shape)


def merge_and_project(layer, core, parts, mine, other, chips):
    rows = parts[0].shape[1] - STATS
    return pl.pallas_call(
        functools.partial(merge_kernel, layer),
        in_specs=[pl.BlockSpec(memory_space=pltpu.SMEM)] + in_vmem(len(parts) + 2),
        out_specs=in_vmem(1)[0],
        out_shape=vmem_out((chips, rows // chips, mine.shape[2])),
        compiler_params=pltpu.CompilerParams(vmem_limit_bytes=8192 * 1024),
        name="merge_and_project",
    )(core, *held_in_vmem(*parts, mine, other))


def finish_kernel(layer, part_ref, residual_ref, out_gain_ref, query_gain_ref, *out_refs):
    summed = jnp.sum(part_ref[...].astype(F32), axis=0)
    change = scaled(summed, out_gain_ref[layer : layer + 1, :])
    residual = (residual_ref[...].astype(F32) + change).astype(BF16)
    out_refs[0][...] = residual
    if layer + 1 < LAYERS:
        normed = scaled(residual.astype(F32), query_gain_ref[layer + 1 : layer + 2, :]).astype(BF16)
        for peer in range(out_refs[1].shape[0]):
            out_refs[1][peer] = normed


def finish(layer, parts, residual, out_gain, query_gain):
    shapes = [residual.shape]
    if layer + 1 < LAYERS:
        shapes.append(parts.shape)
    return pl.pallas_call(
        functools.partial(finish_kernel, layer),
        in_specs=in_vmem(4),
        out_specs=in_vmem(len(shapes)),
        out_shape=[jax.ShapeDtypeStruct(shapes[0], BF16)] + [pltpu.HBM(shape, BF16) for shape in shapes[1:]],
        compiler_params=pltpu.CompilerParams(vmem_limit_bytes=4096 * 1024),
        name="finish",
    )(*held_in_vmem(parts, residual, out_gain, query_gain))


def exchange(value, axis):
    return lax.all_to_all(value, axis, split_axis=0, concat_axis=0, tiled=True)


def shifted(value, distance, size):
    return lax.ppermute(value, STAGES, [(z, (z + distance) % size) for z in range(size)])


def swap(value):
    return lax.ppermute(value, "core", [(0, 1), (1, 0)])


def beside(value, quarters):
    return lax.ppermute(value, "quarter", [(q, q ^ 1) for q in range(quarters)])


def after(value, *others):
    return lax.optimization_barrier((value, *others))[0]


def near_step(own, size):
    low, high = halves(own)
    return shifted(own, 1, size), shifted(own, -1, size), shifted(low, -2, size), shifted(high, 2, size)


def layers(
    target,
    source,
    source_gain,
    query_gain,
    out_gain,
    query_weight,
    key_weight,
    value_weight,
    out_weight,
):
    quarters = lax.axis_size("quarter")
    chips = quarters * lax.axis_size("kv")
    stages = lax.axis_size("far") * lax.axis_size("near")
    core = lax.axis_index("core").astype(jnp.int32).reshape(1)
    width = key_weight.shape[2]

    columns = source_columns(source, source_gain[None], key_weight, value_weight, quarters)
    columns = columns.reshape(quarters * 2, 3 * width, -1)
    held = exchange(columns, GROUP)
    first, later = split(held, lax.axis_size("far"))
    own = exchange(first, "far")
    normed = after(first_norm(target, query_gain, chips), own)
    pieces = near_step(own, stages)
    query_other = swap(query_weight)
    out_other = swap(out_weight)
    rows = exchange(normed, CHIPS)
    mine = project_queries(0, core, rows, query_weight, query_other, quarters, pltpu.HBM)
    near_later = lax.all_gather(after(later, mine), STAGES, axis=0, tiled=True)
    near = join(own, *after(pieces, mine))
    far = swap(near)
    queries = exchange(mine, "quarter")
    (parts,) = attend(core, [queries], [near], [far])
    parts, out_other = lax.optimization_barrier((parts, out_other))
    parts = exchange(parts, "quarter")
    projected = merge_and_project(0, core, [parts], out_weight, out_other, chips)
    arrived = exchange(projected, CHIPS)
    residual, normed = finish(0, arrived, target, out_gain, query_gain)

    rows = exchange(normed, CHIPS)
    far_later = swap(near_later)
    mine = project_queries(1, core, rows, query_weight, query_other, 1, pltpu.VMEM)
    theirs = beside(mine, quarters)
    kept, sent = attend(core, [mine, theirs], [near_later], [far_later])
    came = beside(sent, quarters)
    projected = merge_and_project(1, core, [kept, came], out_weight, out_other, chips)
    arrived = exchange(projected, CHIPS)
    (residual,) = finish(1, arrived, residual, out_gain, query_gain)
    return residual


def solution(mesh):
    groups, stages, devices = mesh.devices.shape
    near = 4
    own = Mesh(
        mesh.devices.reshape(groups, stages // near, near, KVH, devices // (2 * KVH), 2),
        ("grp", "far", "near", "kv", "quarter", "core"),
    )
    every = ("grp", "far", "near", "kv", "quarter", "core")
    tp = ("kv", "quarter", "core")
    in_specs = (
        P(every, None),
        P(("grp", "far", "near"), None),
        P(),
        P(),
        P(),
        P(None, None, tp),
        P(None, None, tp),
        P(None, None, tp),
        P(None, tp, None),
    )
    return jax.shard_map(layers, mesh=own, in_specs=in_specs, out_specs=P(every, None), check_vma=False)
```

```python
import functools

import jax
import jax.numpy as jnp
from jax import lax
from jax.experimental import pallas as pl
from jax.experimental.pallas import tpu as pltpu
from jax.sharding import Mesh
from jax.sharding import PartitionSpec as P


KVH = 2
LAYERS = 2
EPSILON = 1e-06
STATS = 16

CHIPS = ("kv", "quarter")
GROUP = ("quarter", "core")
BF16 = jnp.bfloat16
F32 = jnp.float32


def dot(a, b, contract=((1,), (0,))):
    return lax.dot_general(a, b, (contract, ((), ())), preferred_element_type=F32)


def scaled(values, gain):
    inverse = lax.rsqrt(jnp.mean(values * values, axis=-1, keepdims=True) + EPSILON)
    return values * inverse * gain


def held_in_vmem(*arrays):
    return [pltpu.with_memory_space_constraint(a, pltpu.VMEM) for a in arrays]


def vmem_out(shape):
    return pltpu.VMEM(tuple(shape), BF16)


def in_vmem(count):
    return [pl.BlockSpec(memory_space=pltpu.VMEM)] * count


def source_kernel(source_ref, gain_ref, key_ref, value_ref, out_ref, weight_ref):
    width = key_ref.shape[1]

    @pl.when(pl.program_id(0) == 0)
    def _():
        for layer in range(LAYERS):
            weight_ref[layer * width : (layer + 1) * width, :] = key_ref[layer]
            weight_ref[(LAYERS + layer) * width : (LAYERS + layer + 1) * width, :] = value_ref[layer]

    normed = scaled(source_ref[...].astype(F32), gain_ref[...]).astype(BF16)
    columns = dot(weight_ref[...], normed, ((1,), (1,))).astype(BF16)
    out_ref[...] = columns.reshape(out_ref.shape)


def source_columns(source, gain, key_weight, value_weight, quarters):
    rows, features = source.shape
    key_weight = jnp.swapaxes(key_weight, 1, 2)
    value_weight = jnp.swapaxes(value_weight, 1, 2)
    width = key_weight.shape[1]
    block = rows // quarters
    shape = (quarters, 2, LAYERS * width, block)
    operands = (source, gain, key_weight, value_weight)
    return pl.pallas_call(
        source_kernel,
        grid=(quarters,),
        in_specs=[
            pl.BlockSpec((block, features), lambda i: (i, 0)),
            pl.BlockSpec((1, features), lambda i: (0, 0)),
            pl.BlockSpec(key_weight.shape, lambda i: (0, 0, 0)),
            pl.BlockSpec(value_weight.shape, lambda i: (0, 0, 0)),
        ],
        out_specs=pl.BlockSpec((1, *shape[1:]), lambda i: (i, 0, 0, 0)),
        out_shape=pltpu.HBM(shape, BF16),
        scratch_shapes=[pltpu.VMEM((2 * LAYERS * width, features), BF16)],
        compiler_params=pltpu.CompilerParams(vmem_limit_bytes=12288 * 1024),
        name="source_columns",
    )(*[pltpu.with_memory_space_constraint(a, pltpu.HBM) for a in operands])


def norm_kernel(rows_ref, gain_ref, out_ref):
    normed = scaled(rows_ref[...].astype(F32), gain_ref[:1, :]).astype(BF16)
    for peer in range(out_ref.shape[0]):
        out_ref[peer] = normed


def first_norm(rows, gain, chips):
    return pl.pallas_call(
        norm_kernel,
        in_specs=in_vmem(2),
        out_specs=in_vmem(1)[0],
        out_shape=pltpu.HBM((chips, *rows.shape), BF16),
        compiler_params=pltpu.CompilerParams(vmem_limit_bytes=4096 * 1024),
        name="first_norm",
    )(*held_in_vmem(rows, gain))


def query_kernel(core_ref, rows_ref, mine_ref, other_ref, out_ref):
    chips, block, features = rows_ref.shape
    rows = rows_ref[...].reshape(chips * block, features)
    mine = dot(rows, mine_ref[0]).astype(BF16)
    other = dot(rows, other_ref[0]).astype(BF16)
    first = core_ref[0] == 0
    width = mine.shape[1]
    low = jnp.where(first, mine, other)
    high = jnp.where(first, other, mine)
    for peer in range(out_ref.shape[0]):
        out_ref[peer, :, :width] = low
        out_ref[peer, :, width:] = high


def project_queries(layer, core, rows, mine, other, copies):
    chips, block, features = rows.shape
    width = mine.shape[2]
    weight = pl.BlockSpec((1, features, width), lambda i: (layer, 0, 0))
    shape = (copies, chips * block, 2 * width)
    return pl.pallas_call(
        query_kernel,
        grid=(1,),
        in_specs=[
            pl.BlockSpec(memory_space=pltpu.SMEM),
            pl.BlockSpec(memory_space=pltpu.VMEM),
            weight,
            weight,
        ],
        out_specs=pl.BlockSpec(shape, lambda i: (0, 0, 0)),
        out_shape=pltpu.HBM(shape, BF16),
        compiler_params=pltpu.CompilerParams(vmem_limit_bytes=8192 * 1024),
        name="project_queries",
    )(core, *held_in_vmem(rows), *[pltpu.with_memory_space_constraint(a, pltpu.HBM) for a in (mine, other)])


def attend_kernel(groups, pieces, core_ref, *refs):
    query_refs, refs = refs[:groups], refs[groups:]
    mine_refs, other_refs = refs[:pieces], refs[pieces : 2 * pieces]
    out_refs, score_ref = refs[2 * pieces : -1], refs[-1]
    heads, rows, width = query_refs[0].shape
    queries = [ref[...].reshape(heads * rows, width) for ref in query_refs]
    queries = queries[0] if groups == 1 else jnp.concatenate(queries, axis=0)
    scale = width ** (-0.5)

    def pairs(piece_refs):
        for ref in piece_refs:
            for b in range(0, ref.shape[0], 2):
                yield jnp.concatenate([ref[b], ref[b + 1]], axis=1)

    def work(key_refs, value_refs):
        peak, at, spans = None, 0, []
        for keys in pairs(key_refs):
            scores = dot(queries, keys) * scale
            spans.append(slice(at, at + keys.shape[1]))
            score_ref[:, spans[-1]] = scores
            at += keys.shape[1]
            top = jnp.max(scores, axis=1, keepdims=True)
            peak = top if peak is None else jnp.maximum(peak, top)
        total, mixed = None, None
        for span, values in zip(spans, pairs(value_refs)):
            weights = jnp.exp(score_ref[:, span] - peak)
            part = jnp.sum(weights, axis=1, keepdims=True)
            share = dot(weights.astype(BF16), values, ((1,), (1,)))
            total = part if total is None else total + part
            mixed = share if mixed is None else mixed + share
        attended = (mixed / total).astype(BF16)
        level = peak + jnp.log(total)
        high = level.astype(BF16).astype(F32)
        low = level - high
        for h in range(heads * groups):
            out_ref, own = out_refs[h // heads], slice(h * rows, (h + 1) * rows)
            out_ref[h % heads, :rows, :] = attended[own]
            for part, at in ((high, 0), (low, rows)):
                column = jnp.broadcast_to(part[own], (rows, rows))
                out_ref[h % heads, rows:, at : at + rows] = column.T[:STATS].astype(BF16)

    @pl.when(core_ref[0] == 0)
    def _():
        work(mine_refs, other_refs)

    @pl.when(core_ref[0] != 0)
    def _():
        work(other_refs, mine_refs)


def attend(core, queries, mine, other, placed):
    heads, rows, width = queries[0].shape
    groups = len(queries)
    span = sum(piece.shape[0] * piece.shape[2] for piece in mine)
    return pl.pallas_call(
        functools.partial(attend_kernel, groups, len(mine)),
        in_specs=[pl.BlockSpec(memory_space=pltpu.SMEM)] + in_vmem(groups + 2 * len(mine)),
        out_specs=in_vmem(groups),
        out_shape=[placed((heads, rows + STATS, width), BF16)] * groups,
        scratch_shapes=[pltpu.VMEM((groups * heads * rows, span), F32)],
        compiler_params=pltpu.CompilerParams(vmem_limit_bytes=16384 * 1024),
        name="attend",
    )(core, *held_in_vmem(*queries), *[pltpu.with_memory_space_constraint(a, pltpu.HBM) for a in (*mine, *other)])


def split_kernel(held_ref, *layer_refs):
    devices, width, _ = held_ref.shape
    width //= LAYERS
    for device in range(devices):
        columns = slice(device * width, (device + 1) * width)
        for layer, ref in enumerate(layer_refs):
            ref[0, columns, :] = held_ref[device, layer * width : (layer + 1) * width, :]


def split(held):
    devices, width, block = held.shape
    shape = (1, devices * width // LAYERS, block)
    return pl.pallas_call(
        split_kernel,
        in_specs=in_vmem(1),
        out_specs=in_vmem(LAYERS),
        out_shape=[vmem_out(shape)] + [pltpu.HBM(shape, BF16)] * (LAYERS - 1),
        compiler_params=pltpu.CompilerParams(vmem_limit_bytes=2048 * 1024),
        name="split",
    )(*held_in_vmem(held))


def join_kernel(distance, stage_ref, mine_ref, came_ref, out_ref):
    count = mine_ref.shape[0]
    bit = stage_ref[0] & distance

    @pl.when(bit == 0)
    def _():
        out_ref[:count] = mine_ref[...]
        out_ref[count:] = came_ref[...]

    @pl.when(bit != 0)
    def _():
        out_ref[:count] = came_ref[...]
        out_ref[count:] = mine_ref[...]


def join(distance, stage, mine, came, placed):
    count, *rest = mine.shape
    return pl.pallas_call(
        functools.partial(join_kernel, distance),
        in_specs=[pl.BlockSpec(memory_space=pltpu.SMEM)] + in_vmem(2),
        out_specs=in_vmem(1)[0],
        out_shape=placed((2 * count, *rest), BF16),
        compiler_params=pltpu.CompilerParams(vmem_limit_bytes=2048 * 1024),
        name="join",
    )(stage, mine, came)


def merge_kernel(layer, core_ref, *refs):
    part_refs, (mine_ref, other_ref, out_ref) = refs[:-3], refs[-3:]
    parts = [ref.at[s] for ref in part_refs for s in range(ref.shape[0])]
    rows = parts[0].shape[0] - STATS
    levels = []
    for part in parts:
        stats = part[rows:, :].astype(F32)
        line = stats[:1, :rows] + stats[:1, rows:]
        levels.append(jnp.broadcast_to(line, (rows, rows)).T)
    peak = levels[0]
    for level in levels[1:]:
        peak = jnp.maximum(peak, level)
    shares = [jnp.exp(level - peak) for level in levels]
    total = shares[0]
    for share in shares[1:]:
        total = total + share
    half = mine_ref.shape[1]
    halves = []
    for at in (0, half):
        mixed = None
        for part, share in zip(parts, shares):
            term = part[:rows, at : at + half].astype(F32) * share
            mixed = term if mixed is None else mixed + term
        halves.append((mixed / total).astype(BF16))
    first = core_ref[0] == 0
    mine = jnp.where(first, halves[0], halves[1])
    other = jnp.where(first, halves[1], halves[0])
    projected = dot(mine, mine_ref[layer]) + dot(other, other_ref[layer])
    out_ref[...] = projected.astype(BF16).reshape(out_ref.shape)


def merge_and_project(layer, core, parts, mine, other, chips, placed):
    rows = parts[0].shape[1] - STATS
    return pl.pallas_call(
        functools.partial(merge_kernel, layer),
        in_specs=[pl.BlockSpec(memory_space=pltpu.SMEM)] + in_vmem(len(parts) + 2),
        out_specs=in_vmem(1)[0],
        out_shape=placed((chips, rows // chips, mine.shape[2]), BF16),
        compiler_params=pltpu.CompilerParams(vmem_limit_bytes=8192 * 1024),
        name="merge_and_project",
    )(core, *held_in_vmem(*parts, mine, other))


def finish_kernel(layer, part_ref, residual_ref, out_gain_ref, query_gain_ref, *out_refs):
    summed = jnp.sum(part_ref[...].astype(F32), axis=0)
    change = scaled(summed, out_gain_ref[layer : layer + 1, :])
    residual = (residual_ref[...].astype(F32) + change).astype(BF16)
    out_refs[0][...] = residual
    if layer + 1 < LAYERS:
        normed = scaled(residual.astype(F32), query_gain_ref[layer + 1 : layer + 2, :]).astype(BF16)
        for peer in range(out_refs[1].shape[0]):
            out_refs[1][peer] = normed


def finish(layer, parts, residual, out_gain, query_gain):
    shapes = [residual.shape]
    if layer + 1 < LAYERS:
        shapes.append(parts.shape)
    return pl.pallas_call(
        functools.partial(finish_kernel, layer),
        in_specs=in_vmem(4),
        out_specs=in_vmem(len(shapes)),
        out_shape=[jax.ShapeDtypeStruct(shapes[0], BF16)] + [pltpu.HBM(shape, BF16) for shape in shapes[1:]],
        compiler_params=pltpu.CompilerParams(vmem_limit_bytes=4096 * 1024),
        name="finish",
    )(*held_in_vmem(parts, residual, out_gain, query_gain))


def exchange(value, axis):
    return lax.all_to_all(value, axis, split_axis=0, concat_axis=0, tiled=True)


def passed(value, distance, stages):
    pairs = [
        (2 * stage + core, 2 * ((stage + (distance, -distance)[core]) % stages) + core)
        for stage in range(stages)
        for core in range(2)
    ]
    return lax.ppermute(value, ("sp", "core"), pairs)


def swap(value):
    return lax.ppermute(value, "core", [(0, 1), (1, 0)])


def after(value, *others):
    return lax.optimization_barrier((value, *others))[0]


def layers(
    target,
    source,
    source_gain,
    query_gain,
    out_gain,
    query_weight,
    key_weight,
    value_weight,
    out_weight,
):
    quarters = lax.axis_size("quarter")
    chips = quarters * lax.axis_size("kv")
    stages = lax.axis_size("sp")
    core = lax.axis_index("core").astype(jnp.int32).reshape(1)
    stage = lax.axis_index("sp").astype(jnp.int32).reshape(1)
    width = key_weight.shape[2]
    distances = [stages >> bit for bit in range(1, stages.bit_length())]

    columns = source_columns(source, source_gain[None], key_weight, value_weight, quarters)
    columns = columns.reshape(quarters * 2, LAYERS * width, -1)
    held = exchange(columns, GROUP)
    first, later = split(held)
    query_other = swap(query_weight)
    out_other = swap(out_weight)
    normed = after(first_norm(target, query_gain, chips), held)

    near = first
    for index, distance in enumerate(distances):
        came = passed(near, distance, stages)
        if index + 1 < len(distances):
            near = join(distances[index], stage, near, came, pltpu.VMEM)
    far = [swap(near)]
    far.append(swap(came))
    near = [near, came]

    residual = target
    for layer in range(LAYERS):
        last = layer + 1 == LAYERS
        rows = exchange(normed, CHIPS)
        if last:
            next_near = join(distances[2], stage, next_near, after(came, normed), pltpu.HBM)
            came = passed(next_near, distances[3], stages)
            far = [swap(next_near)]
            near = [next_near, came]
        mine = project_queries(layer, core, rows, query_weight, query_other, quarters)
        queries = exchange(mine, "quarter")
        if last:
            far.append(swap(after(came, mine)))
        else:
            came = passed(after(later, near[1]), distances[0], stages)
        placed = pltpu.VMEM if last else pltpu.HBM
        (parts,) = attend(core, [queries], near, far, placed)
        if not last:
            parts, out_other = lax.optimization_barrier((parts, out_other))
            next_near = join(distances[0], stage, later, after(came, parts), pltpu.HBM)
            came = passed(next_near, distances[1], stages)
        parts = exchange(parts, "quarter")
        projected = merge_and_project(layer, core, [parts], out_weight, out_other, chips, placed)
        if not last:
            next_near = join(distances[1], stage, next_near, after(came, projected), pltpu.HBM)
            came = passed(next_near, distances[2], stages)
        arrived = exchange(projected, CHIPS)
        done = finish(layer, arrived, residual, out_gain, query_gain)
        residual = done[0]
        normed = done[-1]
    return residual


def solution(mesh):
    groups, stages, devices = mesh.devices.shape
    own = Mesh(
        mesh.devices.reshape(groups, stages, KVH, devices // (2 * KVH), 2),
        ("grp", "sp", "kv", "quarter", "core"),
    )
    every = ("grp", "sp", "kv", "quarter", "core")
    tp = ("kv", "quarter", "core")
    in_specs = (
        P(every, None),
        P(("grp", "sp"), None),
        P(),
        P(),
        P(),
        P(None, None, tp),
        P(None, None, tp),
        P(None, None, tp),
        P(None, tp, None),
    )
    return jax.shard_map(layers, mesh=own, in_specs=in_specs, out_specs=P(every, None), check_vma=False)
```

```python
import functools

import jax
import jax.numpy as jnp
from jax import lax
from jax.experimental import pallas as pl
from jax.experimental.pallas import tpu as pltpu
from jax.sharding import Mesh
from jax.sharding import PartitionSpec as P


KVH = 2
LAYERS = 2
EPSILON = 1e-06
STATS = 16

CHIPS = ("kv", "quarter")
GROUP = ("quarter", "core")
STAGES = ("far", "near")
BF16 = jnp.bfloat16
F32 = jnp.float32


def dot(a, b, contract=((1,), (0,))):
    return lax.dot_general(a, b, (contract, ((), ())), preferred_element_type=F32)


def scaled(values, gain):
    inverse = lax.rsqrt(jnp.mean(values * values, axis=-1, keepdims=True) + EPSILON)
    return values * inverse * gain


def held_in_vmem(*arrays):
    return [pltpu.with_memory_space_constraint(a, pltpu.VMEM) for a in arrays]


def vmem_out(shape):
    return pltpu.VMEM(tuple(shape), BF16)


def in_vmem(count):
    return [pl.BlockSpec(memory_space=pltpu.VMEM)] * count


def source_kernel(source_ref, gain_ref, key_ref, value_ref, out_ref, weight_ref):
    width = key_ref.shape[1]
    quarters = out_ref.shape[0]
    step = pl.program_id(0)

    @pl.when(step == 0)
    def _():
        for layer in range(LAYERS):
            weight_ref[layer * width : (layer + 1) * width, :] = key_ref[layer]
            weight_ref[(LAYERS + layer) * width : (LAYERS + layer + 1) * width, :] = value_ref[layer]

    normed = scaled(source_ref[...].astype(F32), gain_ref[...]).astype(BF16)
    columns = dot(weight_ref[...], normed, ((1,), (1,))).astype(BF16)
    for block in range(quarters):

        @pl.when(step == block)
        def _():
            half, at = block // 2, width * (1 + block % 2)
            for core in range(2):
                first = columns[2 * core * width : (2 * core + 1) * width]
                later = columns[(2 * core + 1) * width : (2 * core + 2) * width]
                out_ref[block, core, :width, :] = first
                for quarter in range(half, quarters, 2):
                    out_ref[quarter, core, at : at + width, :] = later


def source_columns(source, gain, key_weight, value_weight, quarters):
    rows, features = source.shape
    key_weight = jnp.swapaxes(key_weight, 1, 2)
    value_weight = jnp.swapaxes(value_weight, 1, 2)
    width = key_weight.shape[1]
    block = rows // quarters
    shape = (quarters, 2, 3 * width, block)
    operands = (source, gain, key_weight, value_weight)
    return pl.pallas_call(
        source_kernel,
        grid=(quarters,),
        in_specs=[
            pl.BlockSpec((block, features), lambda i: (i, 0)),
            pl.BlockSpec((1, features), lambda i: (0, 0)),
            pl.BlockSpec(key_weight.shape, lambda i: (0, 0, 0)),
            pl.BlockSpec(value_weight.shape, lambda i: (0, 0, 0)),
        ],
        out_specs=pl.BlockSpec(shape, lambda i: (0, 0, 0, 0)),
        out_shape=pltpu.HBM(shape, BF16),
        scratch_shapes=[pltpu.VMEM((2 * LAYERS * width, features), BF16)],
        compiler_params=pltpu.CompilerParams(vmem_limit_bytes=12288 * 1024),
        name="source_columns",
    )(*[pltpu.with_memory_space_constraint(a, pltpu.HBM) for a in operands])


def norm_kernel(rows_ref, gain_ref, out_ref):
    normed = scaled(rows_ref[...].astype(F32), gain_ref[:1, :]).astype(BF16)
    for peer in range(out_ref.shape[0]):
        out_ref[peer] = normed


def first_norm(rows, gain, chips):
    return pl.pallas_call(
        norm_kernel,
        in_specs=in_vmem(2),
        out_specs=in_vmem(1)[0],
        out_shape=pltpu.HBM((chips, *rows.shape), BF16),
        compiler_params=pltpu.CompilerParams(vmem_limit_bytes=4096 * 1024),
        name="first_norm",
    )(*held_in_vmem(rows, gain))


def query_kernel(core_ref, rows_ref, mine_ref, other_ref, out_ref):
    chips, block, features = rows_ref.shape
    rows = rows_ref[...].reshape(chips * block, features)
    mine = dot(rows, mine_ref[0]).astype(BF16)
    other = dot(rows, other_ref[0]).astype(BF16)
    first = core_ref[0] == 0
    width = mine.shape[1]
    low = jnp.where(first, mine, other)
    high = jnp.where(first, other, mine)
    for peer in range(out_ref.shape[0]):
        out_ref[peer, :, :width] = low
        out_ref[peer, :, width:] = high


def project_queries(layer, core, rows, mine, other, copies, placed):
    chips, block, features = rows.shape
    width = mine.shape[2]
    weight = pl.BlockSpec((1, features, width), lambda i: (layer, 0, 0))
    shape = (copies, chips * block, 2 * width)
    return pl.pallas_call(
        query_kernel,
        grid=(1,),
        in_specs=[
            pl.BlockSpec(memory_space=pltpu.SMEM),
            pl.BlockSpec(memory_space=pltpu.VMEM),
            weight,
            weight,
        ],
        out_specs=pl.BlockSpec(shape, lambda i: (0, 0, 0)),
        out_shape=placed(shape, BF16),
        compiler_params=pltpu.CompilerParams(vmem_limit_bytes=8192 * 1024),
        name="project_queries",
    )(core, *held_in_vmem(rows), *[pltpu.with_memory_space_constraint(a, pltpu.HBM) for a in (mine, other)])


def attend_kernel(groups, pieces, core_ref, *refs):
    query_refs, refs = refs[:groups], refs[groups:]
    mine_refs, other_refs = refs[:pieces], refs[pieces : 2 * pieces]
    out_refs, score_ref = refs[2 * pieces : -1], refs[-1]
    heads, rows, width = query_refs[0].shape
    queries = [ref[...].reshape(heads * rows, width) for ref in query_refs]
    queries = queries[0] if groups == 1 else jnp.concatenate(queries, axis=0)
    scale = width ** (-0.5)

    def pairs(piece_refs):
        for ref in piece_refs:
            for b in range(0, ref.shape[0], 2):
                yield jnp.concatenate([ref[b], ref[b + 1]], axis=1)

    def work(key_refs, value_refs):
        peak, at, spans = None, 0, []
        for keys in pairs(key_refs):
            scores = dot(queries, keys) * scale
            spans.append(slice(at, at + keys.shape[1]))
            score_ref[:, spans[-1]] = scores
            at += keys.shape[1]
            top = jnp.max(scores, axis=1, keepdims=True)
            peak = top if peak is None else jnp.maximum(peak, top)
        total, mixed = None, None
        for span, values in zip(spans, pairs(value_refs)):
            weights = jnp.exp(score_ref[:, span] - peak)
            part = jnp.sum(weights, axis=1, keepdims=True)
            share = dot(weights.astype(BF16), values, ((1,), (1,)))
            total = part if total is None else total + part
            mixed = share if mixed is None else mixed + share
        attended = (mixed / total).astype(BF16)
        level = peak + jnp.log(total)
        high = level.astype(BF16).astype(F32)
        low = level - high
        for h in range(heads * groups):
            out_ref, own = out_refs[h // heads], slice(h * rows, (h + 1) * rows)
            out_ref[h % heads, :rows, :] = attended[own]
            for part, at in ((high, 0), (low, rows)):
                column = jnp.broadcast_to(part[own], (rows, rows))
                out_ref[h % heads, rows:, at : at + rows] = column.T[:STATS].astype(BF16)

    @pl.when(core_ref[0] == 0)
    def _():
        work(mine_refs, other_refs)

    @pl.when(core_ref[0] != 0)
    def _():
        work(other_refs, mine_refs)


def attend(core, queries, mine, other):
    heads, rows, width = queries[0].shape
    groups = len(queries)
    span = sum(piece.shape[0] * piece.shape[2] for piece in mine)
    return pl.pallas_call(
        functools.partial(attend_kernel, groups, len(mine)),
        in_specs=[pl.BlockSpec(memory_space=pltpu.SMEM)] + in_vmem(groups + 2 * len(mine)),
        out_specs=in_vmem(groups),
        out_shape=[vmem_out((heads, rows + STATS, width))] * groups,
        scratch_shapes=[pltpu.VMEM((groups * heads * rows, span), F32)],
        compiler_params=pltpu.CompilerParams(vmem_limit_bytes=16384 * 1024),
        name="attend",
    )(core, *held_in_vmem(*queries), *[pltpu.with_memory_space_constraint(a, pltpu.HBM) for a in (*mine, *other)])


def split_kernel(held_ref, first_ref, later_ref):
    devices, width, _ = held_ref.shape
    width //= 3
    for device in range(devices):
        columns = slice(device * width, (device + 1) * width)
        for peer in range(first_ref.shape[0]):
            first_ref[peer, columns, :] = held_ref[device, :width, :]
        for half in range(2):
            at = width * (1 + half)
            later_ref[half, columns, :] = held_ref[device, at : at + width, :]


def split(held, copies):
    devices, width, block = held.shape
    column = devices * width // 3
    return pl.pallas_call(
        split_kernel,
        in_specs=in_vmem(1),
        out_specs=in_vmem(2),
        out_shape=[pltpu.HBM((count, column, block), BF16) for count in (copies, 2)],
        compiler_params=pltpu.CompilerParams(vmem_limit_bytes=2048 * 1024),
        name="split",
    )(*held_in_vmem(held))


def join_kernel(distance, stage_ref, mine_ref, came_ref, out_ref):
    count = mine_ref.shape[0]
    bit = stage_ref[0] & distance

    @pl.when(bit == 0)
    def _():
        out_ref[:count] = mine_ref[...]
        out_ref[count:] = came_ref[...]

    @pl.when(bit != 0)
    def _():
        out_ref[:count] = came_ref[...]
        out_ref[count:] = mine_ref[...]


def join(distance, stage, mine, came, placed):
    count, *rest = mine.shape
    return pl.pallas_call(
        functools.partial(join_kernel, distance),
        in_specs=[pl.BlockSpec(memory_space=pltpu.SMEM)] + in_vmem(2),
        out_specs=in_vmem(1)[0],
        out_shape=placed((2 * count, *rest), BF16),
        compiler_params=pltpu.CompilerParams(vmem_limit_bytes=2048 * 1024),
        name="join",
    )(stage, mine, came)


def merge_kernel(layer, core_ref, *refs):
    part_refs, (mine_ref, other_ref, out_ref) = refs[:-3], refs[-3:]
    parts = [ref.at[s] for ref in part_refs for s in range(ref.shape[0])]
    rows = parts[0].shape[0] - STATS
    levels = []
    for part in parts:
        stats = part[rows:, :].astype(F32)
        line = stats[:1, :rows] + stats[:1, rows:]
        levels.append(jnp.broadcast_to(line, (rows, rows)).T)
    peak = levels[0]
    for level in levels[1:]:
        peak = jnp.maximum(peak, level)
    shares = [jnp.exp(level - peak) for level in levels]
    total = shares[0]
    for share in shares[1:]:
        total = total + share
    half = mine_ref.shape[1]
    halves = []
    for at in (0, half):
        mixed = None
        for part, share in zip(parts, shares):
            term = part[:rows, at : at + half].astype(F32) * share
            mixed = term if mixed is None else mixed + term
        halves.append((mixed / total).astype(BF16))
    first = core_ref[0] == 0
    mine = jnp.where(first, halves[0], halves[1])
    other = jnp.where(first, halves[1], halves[0])
    projected = dot(mine, mine_ref[layer]) + dot(other, other_ref[layer])
    out_ref[...] = projected.astype(BF16).reshape(out_ref.shape)


def merge_and_project(layer, core, parts, mine, other, chips):
    rows = parts[0].shape[1] - STATS
    return pl.pallas_call(
        functools.partial(merge_kernel, layer),
        in_specs=[pl.BlockSpec(memory_space=pltpu.SMEM)] + in_vmem(len(parts) + 2),
        out_specs=in_vmem(1)[0],
        out_shape=vmem_out((chips, rows // chips, mine.shape[2])),
        compiler_params=pltpu.CompilerParams(vmem_limit_bytes=8192 * 1024),
        name="merge_and_project",
    )(core, *held_in_vmem(*parts, mine, other))


def finish_kernel(layer, part_ref, residual_ref, out_gain_ref, query_gain_ref, *out_refs):
    summed = jnp.sum(part_ref[...].astype(F32), axis=0)
    change = scaled(summed, out_gain_ref[layer : layer + 1, :])
    residual = (residual_ref[...].astype(F32) + change).astype(BF16)
    out_refs[0][...] = residual
    if layer + 1 < LAYERS:
        normed = scaled(residual.astype(F32), query_gain_ref[layer + 1 : layer + 2, :]).astype(BF16)
        for peer in range(out_refs[1].shape[0]):
            out_refs[1][peer] = normed


def finish(layer, parts, residual, out_gain, query_gain):
    shapes = [residual.shape]
    if layer + 1 < LAYERS:
        shapes.append(parts.shape)
    return pl.pallas_call(
        functools.partial(finish_kernel, layer),
        in_specs=in_vmem(4),
        out_specs=in_vmem(len(shapes)),
        out_shape=[jax.ShapeDtypeStruct(shapes[0], BF16)] + [pltpu.HBM(shape, BF16) for shape in shapes[1:]],
        compiler_params=pltpu.CompilerParams(vmem_limit_bytes=4096 * 1024),
        name="finish",
    )(*held_in_vmem(parts, residual, out_gain, query_gain))


def exchange(value, axis):
    return lax.all_to_all(value, axis, split_axis=0, concat_axis=0, tiled=True)


def passed(value, distance, stages):
    pairs = [
        (2 * stage + core, 2 * ((stage + (distance, -distance)[core]) % stages) + core)
        for stage in range(stages)
        for core in range(2)
    ]
    return lax.ppermute(value, ("far", "near", "core"), pairs)


def swap(value):
    return lax.ppermute(value, "core", [(0, 1), (1, 0)])


def beside(value, quarters):
    return lax.ppermute(value, "quarter", [(q, q ^ 1) for q in range(quarters)])


def after(value, *others):
    return lax.optimization_barrier((value, *others))[0]


def layers(
    target,
    source,
    source_gain,
    query_gain,
    out_gain,
    query_weight,
    key_weight,
    value_weight,
    out_weight,
):
    quarters = lax.axis_size("quarter")
    chips = quarters * lax.axis_size("kv")
    stages = lax.axis_size("far") * lax.axis_size("near")
    core = lax.axis_index("core").astype(jnp.int32).reshape(1)
    stage = lax.axis_index(STAGES).astype(jnp.int32).reshape(1)
    width = key_weight.shape[2]

    columns = source_columns(source, source_gain[None], key_weight, value_weight, quarters)
    columns = columns.reshape(quarters * 2, 3 * width, -1)
    held = exchange(columns, GROUP)
    first, later = split(held, lax.axis_size("far"))
    own = exchange(first, "far")
    normed = after(first_norm(target, query_gain, chips), own)
    came = passed(own, 2, stages)
    near = join(2, stage, own, came, pltpu.VMEM)
    came = passed(near, 1, stages)
    far = [swap(near)]
    far.append(swap(came))
    near_later = lax.all_gather(after(later, near), STAGES, axis=0, tiled=True)
    near = [near, came]
    query_other = swap(query_weight)
    out_other = swap(out_weight)
    rows = exchange(normed, CHIPS)
    mine = project_queries(0, core, rows, query_weight, query_other, quarters, pltpu.HBM)
    queries = exchange(mine, "quarter")
    (parts,) = attend(core, [queries], near, far)
    parts, out_other = lax.optimization_barrier((parts, out_other))
    parts = exchange(parts, "quarter")
    projected = merge_and_project(0, core, [parts], out_weight, out_other, chips)
    arrived = exchange(projected, CHIPS)
    residual, normed = finish(0, arrived, target, out_gain, query_gain)

    rows = exchange(normed, CHIPS)
    far_later = swap(near_later)
    mine = project_queries(1, core, rows, query_weight, query_other, 1, pltpu.VMEM)
    theirs = beside(mine, quarters)
    kept, sent = attend(core, [mine, theirs], [near_later], [far_later])
    came = beside(sent, quarters)
    projected = merge_and_project(1, core, [kept, came], out_weight, out_other, chips)
    arrived = exchange(projected, CHIPS)
    (residual,) = finish(1, arrived, residual, out_gain, query_gain)
    return residual


def solution(mesh):
    groups, stages, devices = mesh.devices.shape
    near = 4
    own = Mesh(
        mesh.devices.reshape(groups, stages // near, near, KVH, devices // (2 * KVH), 2),
        ("grp", "far", "near", "kv", "quarter", "core"),
    )
    every = ("grp", "far", "near", "kv", "quarter", "core")
    tp = ("kv", "quarter", "core")
    in_specs = (
        P(every, None),
        P(("grp", "far", "near"), None),
        P(),
        P(),
        P(),
        P(None, None, tp),
        P(None, None, tp),
        P(None, None, tp),
        P(None, tp, None),
    )
    return jax.shard_map(layers, mesh=own, in_specs=in_specs, out_specs=P(every, None), check_vma=False)
```

```python
import functools

import jax
import jax.numpy as jnp
from jax import lax
from jax.experimental import pallas as pl
from jax.experimental.pallas import tpu as pltpu
from jax.sharding import Mesh
from jax.sharding import PartitionSpec as P


KVH = 2
LAYERS = 2
EPSILON = 1e-06
STATS = 16

CHIPS = ("kv", "quarter")
GROUP = ("quarter", "core")
STAGES = ("far", "near")
BF16 = jnp.bfloat16
F32 = jnp.float32


def dot(a, b, contract=((1,), (0,))):
    return lax.dot_general(a, b, (contract, ((), ())), preferred_element_type=F32)


def scaled(values, gain):
    inverse = lax.rsqrt(jnp.mean(values * values, axis=-1, keepdims=True) + EPSILON)
    return values * inverse * gain


def held_in_vmem(*arrays):
    return [pltpu.with_memory_space_constraint(a, pltpu.VMEM) for a in arrays]


def vmem_out(shape):
    return pltpu.VMEM(tuple(shape), BF16)


def in_vmem(count):
    return [pl.BlockSpec(memory_space=pltpu.VMEM)] * count


def source_kernel(source_ref, gain_ref, key_ref, value_ref, out_ref, weight_ref):
    width = key_ref.shape[1]
    quarters = out_ref.shape[0]
    step = pl.program_id(0)

    @pl.when(step == 0)
    def _():
        for layer in range(LAYERS):
            weight_ref[layer * width : (layer + 1) * width, :] = key_ref[layer]
            weight_ref[(LAYERS + layer) * width : (LAYERS + layer + 1) * width, :] = value_ref[layer]

    normed = scaled(source_ref[...].astype(F32), gain_ref[...]).astype(BF16)
    columns = dot(weight_ref[...], normed, ((1,), (1,))).astype(BF16)
    for block in range(quarters):

        @pl.when(step == block)
        def _():
            half, at = block // 2, width * (1 + block % 2)
            for core in range(2):
                first = columns[2 * core * width : (2 * core + 1) * width]
                later = columns[(2 * core + 1) * width : (2 * core + 2) * width]
                out_ref[block, core, :width, :] = first
                for quarter in range(half, quarters, 2):
                    out_ref[quarter, core, at : at + width, :] = later


def source_columns(source, gain, key_weight, value_weight, quarters):
    rows, features = source.shape
    key_weight = jnp.swapaxes(key_weight, 1, 2)
    value_weight = jnp.swapaxes(value_weight, 1, 2)
    width = key_weight.shape[1]
    block = rows // quarters
    shape = (quarters, 2, 3 * width, block)
    operands = (source, gain, key_weight, value_weight)
    return pl.pallas_call(
        source_kernel,
        grid=(quarters,),
        in_specs=[
            pl.BlockSpec((block, features), lambda i: (i, 0)),
            pl.BlockSpec((1, features), lambda i: (0, 0)),
            pl.BlockSpec(key_weight.shape, lambda i: (0, 0, 0)),
            pl.BlockSpec(value_weight.shape, lambda i: (0, 0, 0)),
        ],
        out_specs=pl.BlockSpec(shape, lambda i: (0, 0, 0, 0)),
        out_shape=pltpu.HBM(shape, BF16),
        scratch_shapes=[pltpu.VMEM((2 * LAYERS * width, features), BF16)],
        compiler_params=pltpu.CompilerParams(vmem_limit_bytes=12288 * 1024),
        name="source_columns",
    )(*[pltpu.with_memory_space_constraint(a, pltpu.HBM) for a in operands])


def norm_kernel(rows_ref, gain_ref, out_ref):
    out_ref[0] = scaled(rows_ref[...].astype(F32), gain_ref[:1, :]).astype(BF16)


def first_norm(rows, gain):
    return pl.pallas_call(
        norm_kernel,
        in_specs=in_vmem(2),
        out_specs=in_vmem(1)[0],
        out_shape=vmem_out((1, *rows.shape)),
        compiler_params=pltpu.CompilerParams(vmem_limit_bytes=4096 * 1024),
        name="first_norm",
    )(*held_in_vmem(rows, gain))


def query_kernel(order, core_ref, rows_ref, mine_ref, other_ref, out_ref):
    rows = jnp.concatenate([rows_ref[chip] for chip in order], axis=0)
    mine = dot(rows, mine_ref[0]).astype(BF16)
    other = dot(rows, other_ref[0]).astype(BF16)
    first = core_ref[0] == 0
    width = mine.shape[1]
    low = jnp.where(first, mine, other)
    high = jnp.where(first, other, mine)
    for peer in range(out_ref.shape[0]):
        out_ref[peer, :, :width] = low
        out_ref[peer, :, width:] = high


def project_queries(layer, core, rows, order, mine, other, copies, placed):
    chips, block, features = rows.shape
    width = mine.shape[2]
    weight = pl.BlockSpec((1, features, width), lambda i: (layer, 0, 0))
    shape = (copies, chips * block, 2 * width)
    return pl.pallas_call(
        functools.partial(query_kernel, tuple(order)),
        grid=(1,),
        in_specs=[
            pl.BlockSpec(memory_space=pltpu.SMEM),
            pl.BlockSpec(memory_space=pltpu.VMEM),
            weight,
            weight,
        ],
        out_specs=pl.BlockSpec(shape, lambda i: (0, 0, 0)),
        out_shape=placed(shape, BF16),
        compiler_params=pltpu.CompilerParams(vmem_limit_bytes=8192 * 1024),
        name="project_queries",
    )(core, *held_in_vmem(rows), *[pltpu.with_memory_space_constraint(a, pltpu.HBM) for a in (mine, other)])


def attend_kernel(groups, pieces, core_ref, *refs):
    query_refs, refs = refs[:groups], refs[groups:]
    mine_refs, other_refs = refs[:pieces], refs[pieces : 2 * pieces]
    out_refs, score_ref = refs[2 * pieces : -1], refs[-1]
    heads, rows, width = query_refs[0].shape
    queries = [ref[...].reshape(heads * rows, width) for ref in query_refs]
    queries = queries[0] if groups == 1 else jnp.concatenate(queries, axis=0)
    scale = width ** (-0.5)

    def pairs(piece_refs):
        for ref in piece_refs:
            for b in range(0, ref.shape[0], 2):
                yield jnp.concatenate([ref[b], ref[b + 1]], axis=1)

    def work(key_refs, value_refs):
        peak, at, spans = None, 0, []
        for keys in pairs(key_refs):
            scores = dot(queries, keys) * scale
            spans.append(slice(at, at + keys.shape[1]))
            score_ref[:, spans[-1]] = scores
            at += keys.shape[1]
            top = jnp.max(scores, axis=1, keepdims=True)
            peak = top if peak is None else jnp.maximum(peak, top)
        total, mixed = None, None
        for span, values in zip(spans, pairs(value_refs)):
            weights = jnp.exp(score_ref[:, span] - peak)
            part = jnp.sum(weights, axis=1, keepdims=True)
            share = dot(weights.astype(BF16), values, ((1,), (1,)))
            total = part if total is None else total + part
            mixed = share if mixed is None else mixed + share
        attended = (mixed / total).astype(BF16)
        level = peak + jnp.log(total)
        high = level.astype(BF16).astype(F32)
        low = level - high
        for h in range(heads * groups):
            out_ref, own = out_refs[h // heads], slice(h * rows, (h + 1) * rows)
            out_ref[h % heads, :rows, :] = attended[own]
            for part, at in ((high, 0), (low, rows)):
                column = jnp.broadcast_to(part[own], (rows, rows))
                out_ref[h % heads, rows:, at : at + rows] = column.T[:STATS].astype(BF16)

    @pl.when(core_ref[0] == 0)
    def _():
        work(mine_refs, other_refs)

    @pl.when(core_ref[0] != 0)
    def _():
        work(other_refs, mine_refs)


def attend(core, queries, mine, other):
    heads, rows, width = queries[0].shape
    groups = len(queries)
    span = sum(piece.shape[0] * piece.shape[2] for piece in mine)
    return pl.pallas_call(
        functools.partial(attend_kernel, groups, len(mine)),
        in_specs=[pl.BlockSpec(memory_space=pltpu.SMEM)] + in_vmem(groups + 2 * len(mine)),
        out_specs=in_vmem(groups),
        out_shape=[vmem_out((heads, rows + STATS, width))] * groups,
        scratch_shapes=[pltpu.VMEM((groups * heads * rows, span), F32)],
        compiler_params=pltpu.CompilerParams(vmem_limit_bytes=16384 * 1024),
        name="attend",
    )(core, *held_in_vmem(*queries), *[pltpu.with_memory_space_constraint(a, pltpu.HBM) for a in (*mine, *other)])


def split_kernel(held_ref, first_ref, later_ref):
    devices, width, _ = held_ref.shape
    width //= 3
    for device in range(devices):
        columns = slice(device * width, (device + 1) * width)
        for peer in range(first_ref.shape[0]):
            first_ref[peer, columns, :] = held_ref[device, :width, :]
        for half in range(2):
            at = width * (1 + half)
            later_ref[half, columns, :] = held_ref[device, at : at + width, :]


def split(held, copies):
    devices, width, block = held.shape
    column = devices * width // 3
    return pl.pallas_call(
        split_kernel,
        in_specs=in_vmem(1),
        out_specs=in_vmem(2),
        out_shape=[pltpu.HBM((count, column, block), BF16) for count in (copies, 2)],
        compiler_params=pltpu.CompilerParams(vmem_limit_bytes=2048 * 1024),
        name="split",
    )(*held_in_vmem(held))


def join_kernel(distance, stage_ref, mine_ref, came_ref, out_ref):
    count = mine_ref.shape[0]
    bit = stage_ref[0] & distance

    @pl.when(bit == 0)
    def _():
        out_ref[:count] = mine_ref[...]
        out_ref[count:] = came_ref[...]

    @pl.when(bit != 0)
    def _():
        out_ref[:count] = came_ref[...]
        out_ref[count:] = mine_ref[...]


def join(distance, stage, mine, came, placed):
    count, *rest = mine.shape
    return pl.pallas_call(
        functools.partial(join_kernel, distance),
        in_specs=[pl.BlockSpec(memory_space=pltpu.SMEM)] + in_vmem(2),
        out_specs=in_vmem(1)[0],
        out_shape=placed((2 * count, *rest), BF16),
        compiler_params=pltpu.CompilerParams(vmem_limit_bytes=2048 * 1024),
        name="join",
    )(stage, mine, came)


def merge_kernel(layer, core_ref, *refs):
    part_refs, (mine_ref, other_ref, out_ref) = refs[:-3], refs[-3:]
    parts = [ref.at[s] for ref in part_refs for s in range(ref.shape[0])]
    rows = parts[0].shape[0] - STATS
    levels = []
    for part in parts:
        stats = part[rows:, :].astype(F32)
        line = stats[:1, :rows] + stats[:1, rows:]
        levels.append(jnp.broadcast_to(line, (rows, rows)).T)
    peak = levels[0]
    for level in levels[1:]:
        peak = jnp.maximum(peak, level)
    shares = [jnp.exp(level - peak) for level in levels]
    total = shares[0]
    for share in shares[1:]:
        total = total + share
    half = mine_ref.shape[1]
    halves = []
    for at in (0, half):
        mixed = None
        for part, share in zip(parts, shares):
            term = part[:rows, at : at + half].astype(F32) * share
            mixed = term if mixed is None else mixed + term
        halves.append((mixed / total).astype(BF16))
    first = core_ref[0] == 0
    mine = jnp.where(first, halves[0], halves[1])
    other = jnp.where(first, halves[1], halves[0])
    projected = dot(mine, mine_ref[layer]) + dot(other, other_ref[layer])
    out_ref[...] = projected.astype(BF16).reshape(out_ref.shape)


def merge_and_project(layer, core, parts, mine, other, chips):
    rows = parts[0].shape[1] - STATS
    return pl.pallas_call(
        functools.partial(merge_kernel, layer),
        in_specs=[pl.BlockSpec(memory_space=pltpu.SMEM)] + in_vmem(len(parts) + 2),
        out_specs=in_vmem(1)[0],
        out_shape=vmem_out((chips, rows // chips, mine.shape[2])),
        compiler_params=pltpu.CompilerParams(vmem_limit_bytes=8192 * 1024),
        name="merge_and_project",
    )(core, *held_in_vmem(*parts, mine, other))


def finish_kernel(layer, part_ref, residual_ref, out_gain_ref, query_gain_ref, *out_refs):
    summed = jnp.sum(part_ref[...].astype(F32), axis=0)
    change = scaled(summed, out_gain_ref[layer : layer + 1, :])
    residual = (residual_ref[...].astype(F32) + change).astype(BF16)
    out_refs[0][...] = residual
    if layer + 1 < LAYERS:
        normed = scaled(residual.astype(F32), query_gain_ref[layer + 1 : layer + 2, :]).astype(BF16)
        for peer in range(out_refs[1].shape[0]):
            out_refs[1][peer] = normed


def finish(layer, parts, residual, out_gain, query_gain):
    shapes = [residual.shape]
    if layer + 1 < LAYERS:
        shapes.append(parts.shape)
    return pl.pallas_call(
        functools.partial(finish_kernel, layer),
        in_specs=in_vmem(4),
        out_specs=in_vmem(len(shapes)),
        out_shape=[jax.ShapeDtypeStruct(shapes[0], BF16)] + [pltpu.HBM(shape, BF16) for shape in shapes[1:]],
        compiler_params=pltpu.CompilerParams(vmem_limit_bytes=4096 * 1024),
        name="finish",
    )(*held_in_vmem(parts, residual, out_gain, query_gain))


def exchange(value, axis):
    return lax.all_to_all(value, axis, split_axis=0, concat_axis=0, tiled=True)


def passed(value, distance, axes, size):
    pairs = [
        (2 * at + core, 2 * ((at + (distance, -distance)[core]) % size) + core)
        for at in range(size)
        for core in range(2)
    ]
    return lax.ppermute(value, (*axes, "core"), pairs)


def swap(value):
    return lax.ppermute(value, "core", [(0, 1), (1, 0)])


def beside(value, quarters):
    return lax.ppermute(value, "quarter", [(q, q ^ 1) for q in range(quarters)])


def after(value, *others):
    return lax.optimization_barrier((value, *others))[0]


def layers(
    target,
    source,
    source_gain,
    query_gain,
    out_gain,
    query_weight,
    key_weight,
    value_weight,
    out_weight,
):
    quarters = lax.axis_size("quarter")
    chips = quarters * lax.axis_size("kv")
    stages = lax.axis_size("far") * lax.axis_size("near")
    core = lax.axis_index("core").astype(jnp.int32).reshape(1)
    chip = lax.axis_index(CHIPS).astype(jnp.int32).reshape(1)
    stage = lax.axis_index(STAGES).astype(jnp.int32).reshape(1)
    width = key_weight.shape[2]

    columns = source_columns(source, source_gain[None], key_weight, value_weight, quarters)
    columns = columns.reshape(quarters * 2, 3 * width, -1)
    held = exchange(columns, GROUP)
    first, later = split(held, lax.axis_size("far"))
    own = exchange(first, "far")
    rows = first_norm(target, query_gain)
    for distance in [chips >> bit for bit in range(1, chips.bit_length())]:
        came = passed(rows, distance, CHIPS, chips)
        rows = join(distance, chip, rows, came, pltpu.VMEM)
    width_of_chip = chips.bit_length() - 1
    order = [int(f"{at:0{width_of_chip}b}"[::-1], 2) for at in range(chips)]
    came = passed(own, 2, STAGES, stages)
    near = join(2, stage, own, came, pltpu.VMEM)
    came = passed(near, 1, STAGES, stages)
    far = [swap(near)]
    far.append(swap(came))
    near_later = lax.all_gather(after(later, own), STAGES, axis=0, tiled=True)
    near = [near, came]
    query_other = swap(query_weight)
    out_other = swap(out_weight)
    mine = project_queries(0, core, rows, order, query_weight, query_other, quarters, pltpu.HBM)
    queries = exchange(mine, "quarter")
    (parts,) = attend(core, [queries], near, far)
    parts, out_other = lax.optimization_barrier((parts, out_other))
    parts = exchange(parts, "quarter")
    projected = merge_and_project(0, core, [parts], out_weight, out_other, chips)
    arrived = exchange(projected, CHIPS)
    residual, normed = finish(0, arrived, target, out_gain, query_gain)

    rows = exchange(normed, CHIPS)
    far_later = swap(near_later)
    mine = project_queries(1, core, rows, range(chips), query_weight, query_other, 1, pltpu.VMEM)
    theirs = beside(mine, quarters)
    kept, sent = attend(core, [mine, theirs], [near_later], [far_later])
    came = beside(sent, quarters)
    projected = merge_and_project(1, core, [kept, came], out_weight, out_other, chips)
    arrived = exchange(projected, CHIPS)
    (residual,) = finish(1, arrived, residual, out_gain, query_gain)
    return residual


def solution(mesh):
    groups, stages, devices = mesh.devices.shape
    near = 4
    own = Mesh(
        mesh.devices.reshape(groups, stages // near, near, KVH, devices // (2 * KVH), 2),
        ("grp", "far", "near", "kv", "quarter", "core"),
    )
    every = ("grp", "far", "near", "kv", "quarter", "core")
    tp = ("kv", "quarter", "core")
    in_specs = (
        P(every, None),
        P(("grp", "far", "near"), None),
        P(),
        P(),
        P(),
        P(None, None, tp),
        P(None, None, tp),
        P(None, None, tp),
        P(None, tp, None),
    )
    return jax.shard_map(layers, mesh=own, in_specs=in_specs, out_specs=P(every, None), check_vma=False)
```
